32 devices in a mesh: sp: 8 (over z, y), tp: 4 (over x, core).
Axes of the slice: x: 2, y: 2, z: 4, core: 2. Of those that a mesh axis runs over, the one named last changes fastest.
Arguments:
- inputs: bfloat16 [2, 1024, 2048], P(None, 'sp'), may hold values from -6 to 6
- norm_gain: float32 [2048], replicated, may hold values from 0.1 to 1.9
- query_weight: bfloat16 [2048, 1024], P('sp', 'tp'), may hold values from -0.125 to 0.125
- key_weight: bfloat16 [2048, 256], P('sp', 'tp'), may hold values from -0.125 to 0.125
- value_weight: bfloat16 [2048, 256], P('sp', 'tp'), may hold values from -0.125 to 0.125
- query_gain: float32 [64], replicated, may hold values from 0.1 to 24
- key_gain: float32 [64], replicated, may hold values from 0.1 to 1.9
- forget_cache: float32 [2, 16, 1024], P(None, 'tp'), may hold values from -104 to 0, as said below
- rec_in_weight: bfloat16 [2048, 1024], P('sp', 'tp'), may hold values from -0.125 to 0.125
- rec_gate_weight: bfloat16 [2048, 1024], P('sp', 'tp'), may hold values from -0.125 to 0.125
- conv_weight: bfloat16 [4, 1024], P(None, 'tp'), may hold values from -3 to 3
- decay_gate_weight: bfloat16 [16, 64, 64], P('tp'), may hold values from -0.75 to 0.75
- input_gate_weight: bfloat16 [16, 64, 64], P('tp'), may hold values from -0.75 to 0.75
- decay_param: float32 [1024], P('tp'), may hold values from 4 to 16
- decay_extra: float32 [2, 1024, 1024], P(None, 'sp', 'tp'), may hold values from -2 to 0
- attn_out_gain: float32 [1024], P('tp'), may hold values from 0.1 to 1.9
- rec_out_gain: float32 [1024], P('tp'), may hold values from 0.1 to 1.9
- out_att_weight: bfloat16 [1024, 2048], P('tp'), may hold values from -0.125 to 0.125
- out_rec_weight: bfloat16 [1024, 2048], P('tp'), may hold values from -0.125 to 0.125
Outputs:
- mixed: bfloat16 [2, 1024, 2048], P(None, 'sp', 'tp')
The draws below stay inside these ranges and needn't reach their ends.
Inputs may be any that keep to these rules, and one draw needn't show every extreme that they name: `forget_cache`: Non-increasing along the positions of each sequence and head.
All inputs are finite; a program needn't handle non-finite values.
Results may differ from the reference program's by a relative error of at most 0.012.
The reference program's roundings to bfloat16 on the way count: a program that leaves them out, or rounds other values in their place, can miss the bound.
Values may be sent and summed in bfloat16 or wider, within the bound.
A program may use at most 128 MiB of HBM per device.

```python
import math
import jax
import jax.numpy as jnp
from jax import lax

D = 2048
HEAD_DIM = 64
ATT_HEADS = 16
KV_HEADS = 4
LRU_BLOCK = 64
CONV_TAPS = 4
SEQS = 2
SEQ_TOK = 128
SEQUENCE_LENGTH = 1024
ATT_WIDTH = 1024
KV_WIDTH = 256
LRU_WIDTH = 1024
LRU_BLOCKS = 16


lru_const = 8.0


def spike_log_values(key, total_count):
    key_rows = jax.random.split(key, 2)
    spots = jax.random.randint(key_rows[0], (SEQS, total_count), 0, SEQUENCE_LENGTH)
    kept = jax.random.uniform(key_rows[1], (SEQS, total_count), jnp.float32, 0.5, 0.8)
    hits = (jnp.arange(SEQUENCE_LENGTH)[None, None, :] == spots[:, :, None]).astype(jnp.float32)
    return jnp.sum(hits * jnp.log(kept)[:, :, None], axis=1)


def block_factor(key):
    blocks = SEQUENCE_LENGTH // SEQ_TOK
    multiplier = jnp.exp(jax.random.uniform(key, (SEQS, blocks), jnp.float32, math.log(0.5), math.log(2.0)))
    return jnp.repeat(multiplier, SEQ_TOK, axis=1)


def draw_query_gain(key, part):
    key = jax.random.fold_in(key, 3)
    return 1.0 + 0.18 * jnp.clip(jax.random.normal(key, (HEAD_DIM,), jnp.float32), -4.5, 4.5)


def draw_forget_cache(key, part):
    key_rows = jax.random.split(jax.random.fold_in(key, 7), 6)
    order = jax.random.permutation(key_rows[0], ATT_HEADS)
    slow_rate = 0.6 / SEQUENCE_LENGTH * jax.random.uniform(key_rows[1], (ATT_HEADS,), jnp.float32, 0.5, 1.5)
    fast_len = jnp.exp(jax.random.uniform(key_rows[2], (ATT_HEADS,), jnp.float32, math.log(30.0), math.log(100.0)))
    decay_speed = jnp.where(order < ATT_HEADS // 2, 1.0 / fast_len, slow_rate)
    random_jitter = jax.random.uniform(key_rows[4], (SEQS, ATT_HEADS, SEQUENCE_LENGTH), jnp.float32, 0.5, 1.5)
    multiplier = block_factor(key_rows[3])
    gate_logarithm = -decay_speed[None, :, None] * multiplier[:, None, :] * random_jitter + spike_log_values(key_rows[5], 2)[:, None, :]
    return jnp.cumsum(gate_logarithm, axis=2)


def draw_decay_param(key, part):
    key_rows = jax.random.split(jax.random.fold_in(key, 5), 3)
    order = jax.random.permutation(key_rows[0], LRU_WIDTH)
    slow_rate = 0.3 / (lru_const * SEQUENCE_LENGTH) * jax.random.uniform(key_rows[1], (LRU_WIDTH,), jnp.float32, 0.5, 1.5)
    fast_len = jnp.exp(jax.random.uniform(key_rows[2], (LRU_WIDTH,), jnp.float32, math.log(30.0), math.log(100.0)))
    fast_rate = 1.0 / (0.5 * lru_const * fast_len)
    decay_speed = jnp.where(order < LRU_WIDTH // 2, fast_rate, slow_rate)
    return -jnp.log(jnp.expm1(decay_speed))


def draw_decay_extra(key, part):
    key_rows = jax.random.split(jax.random.fold_in(key, 9), 3)
    multiplier = block_factor(key_rows[0])
    random_jitter = jax.random.uniform(key_rows[1], (SEQS, SEQUENCE_LENGTH, LRU_WIDTH), jnp.float32, 0.5, 1.5)
    return -0.5 / SEQUENCE_LENGTH * multiplier[:, :, None] * random_jitter + spike_log_values(key_rows[2], 2)[:, :, None]


def block_scale(stream_key, dims, pieces, low, largest):
    loudness, own = 1.0, jax.random.fold_in(stream_key, 6)
    for dim, shards_of in pieces:
        draws = jnp.exp(jax.random.uniform(jax.random.fold_in(own, dim), (shards_of,), jnp.float32, low / len(pieces), largest / len(pieces)))
        loudness = loudness * jnp.repeat(draws, dims[dim] // shards_of).reshape([-1 if axis == dim else 1 for axis in range(len(dims))])
    return loudness


def normal_values(stream_key, extent, width, limit, shards=(), kind=jnp.bfloat16):
    result = width * jax.random.normal(stream_key, extent, jnp.float32)
    if shards:
        result = result * block_scale(stream_key, extent, shards, -0.22, 0.18)
    return jnp.clip(result, -limit, limit).astype(kind)


def setup_inputs(seed: int = 0) -> dict:
    key_of = jax.random.split(jax.random.key(seed), 20)
    inputs = normal_values(key_of[0], (SEQS, SEQUENCE_LENGTH, D), 1.0, 6.0, ((1, 8),))
    norm_gain = jnp.clip(1.0 + 0.18 * jax.random.normal(key_of[1], (D,), jnp.float32), 0.1, 1.9)
    query_weight = normal_values(key_of[2], (D, ATT_WIDTH), D ** -0.5, 0.125, ((0, 8), (1, 4)))
    key_weight = normal_values(key_of[3], (D, KV_WIDTH), D ** -0.5, 0.125, ((0, 8), (1, 4)))
    value_weight = normal_values(key_of[4], (D, KV_WIDTH), D ** -0.5, 0.125, ((0, 8), (1, 4)))
    query_gain = draw_query_gain(jax.random.fold_in(key_of[19], 71), 0)
    key_gain = jnp.clip(1.0 + 0.18 * jax.random.normal(key_of[6], (HEAD_DIM,), jnp.float32), 0.1, 1.9)
    forget_cache = draw_forget_cache(jax.random.fold_in(key_of[19], 71), 0)
    rec_in_weight = normal_values(key_of[8], (D, LRU_WIDTH), D ** -0.5, 0.125, ((0, 8), (1, 4)))
    rec_gate_weight = normal_values(key_of[9], (D, LRU_WIDTH), D ** -0.5, 0.125, ((0, 8), (1, 4)))
    conv_weight = normal_values(key_of[10], (CONV_TAPS, LRU_WIDTH), CONV_TAPS ** -0.5, 3.0, ((1, 4),))
    decay_gate_weight = normal_values(key_of[11], (LRU_BLOCKS, LRU_BLOCK, LRU_BLOCK), LRU_BLOCK ** -0.5, 0.75, ((0, 4),))
    input_gate_weight = normal_values(key_of[12], (LRU_BLOCKS, LRU_BLOCK, LRU_BLOCK), LRU_BLOCK ** -0.5, 0.75, ((0, 4),))
    decay_param = draw_decay_param(jax.random.fold_in(key_of[19], 71), 0)
    decay_extra = draw_decay_extra(jax.random.fold_in(key_of[19], 71), 0)
    attn_out_gain = jnp.clip(1.0 + 0.18 * jax.random.normal(key_of[15], (ATT_WIDTH,), jnp.float32), 0.1, 1.9)
    rec_out_gain = jnp.clip(1.0 + 0.18 * jax.random.normal(key_of[16], (LRU_WIDTH,), jnp.float32), 0.1, 1.9)
    out_att_weight = normal_values(key_of[17], (ATT_WIDTH, D), D ** -0.5, 0.125, ((0, 4),))
    out_rec_weight = normal_values(key_of[18], (LRU_WIDTH, D), D ** -0.5, 0.125, ((0, 4),))
    return {"inputs": inputs, "norm_gain": norm_gain, "query_weight": query_weight, "key_weight": key_weight, "value_weight": value_weight, "query_gain": query_gain, "key_gain": key_gain, "forget_cache": forget_cache, "rec_in_weight": rec_in_weight, "rec_gate_weight": rec_gate_weight, "conv_weight": conv_weight, "decay_gate_weight": decay_gate_weight, "input_gate_weight": input_gate_weight, "decay_param": decay_param, "decay_extra": decay_extra, "attn_out_gain": attn_out_gain, "rec_out_gain": rec_out_gain, "out_att_weight": out_att_weight, "out_rec_weight": out_rec_weight}


lru_const = 8.0
norm_eps = 1e-06

def rms_scale(values, gain):
    multiplier = lax.rsqrt(lax.optimization_barrier(jnp.mean(values * values, axis=-1, keepdims=True)) + norm_eps)
    return values * multiplier * gain

def merge_state(earlier, later):
    return (earlier[0] * later[0], later[0] * earlier[1] + later[1])

def attention(queries, key_heads, value_heads, forget_cache):
    seq_count, kv_count, head_group, length, head_dim = queries.shape
    block_size = 512
    while length % block_size:
        block_size //= 2
    scaling = head_dim ** (-0.5)
    gates = forget_cache.reshape(seq_count, kv_count, head_group, length)
    offsets = jnp.arange(block_size, dtype=jnp.int32)

    def one_block(index):
        first = index * block_size
        query_block = lax.dynamic_slice_in_dim(queries, first, block_size, 3).astype(jnp.float32)
        query_gates = lax.dynamic_slice_in_dim(gates, first, block_size, 3)
        query_pos = first + offsets

        def one_step(block_index, carried):
            top_score, totals, accum = carried
            key_first = block_index * block_size
            key_block = lax.dynamic_slice_in_dim(key_heads, key_first, block_size, 2).astype(jnp.float32)
            value_block = lax.dynamic_slice_in_dim(value_heads, key_first, block_size, 2).astype(jnp.float32)
            key_gates = lax.dynamic_slice_in_dim(gates, key_first, block_size, 3)
            scores = jnp.einsum('bhgqd,bhkd->bhgqk', query_block, key_block) * scaling
            scores = scores + query_gates[..., :, None] - key_gates[..., None, :]
            visible = query_pos[:, None] >= (key_first + offsets)[None, :]
            scores = jnp.where(visible, scores, -jnp.inf)
            new_top = jnp.maximum(top_score, lax.optimization_barrier(jnp.max(scores, axis=-1)))
            weights = jnp.exp(scores - new_top[..., None])
            fading = jnp.exp(top_score - new_top)
            rounded = lax.optimization_barrier(weights.astype(jnp.bfloat16)).astype(jnp.float32)
            totals = totals * fading + lax.optimization_barrier(jnp.sum(weights, axis=-1))
            accum = accum * fading[..., None] + jnp.einsum('bhgqk,bhkd->bhgqd', rounded, value_block)
            return (new_top, totals, accum)
        start_state = (jnp.full((seq_count, kv_count, head_group, block_size), -jnp.inf, jnp.float32), jnp.zeros((seq_count, kv_count, head_group, block_size), jnp.float32), jnp.zeros((seq_count, kv_count, head_group, block_size, head_dim), jnp.float32))
        top_score, totals, accum = lax.fori_loop(0, index + 1, one_step, start_state)
        return accum / totals[..., None]
    return lax.map(one_block, jnp.arange(length // block_size, dtype=jnp.int32))

def reference(inputs, norm_gain, query_weight, key_weight, value_weight, query_gain, key_gain, forget_cache, rec_in_weight, rec_gate_weight, conv_weight, decay_gate_weight, input_gate_weight, decay_param, decay_extra, attn_out_gain, rec_out_gain, out_att_weight, out_rec_weight):
    seq_count, length, model_width = inputs.shape
    row_count = seq_count * length
    head_group = ATT_HEADS // KV_HEADS
    flat_rows = inputs.reshape(row_count, model_width).astype(jnp.float32)
    normed = rms_scale(flat_rows, norm_gain).astype(jnp.bfloat16)

    def project(weight):
        return jnp.dot(normed, weight, preferred_element_type=jnp.float32)
    query_proj = project(query_weight)
    key_proj = project(key_weight)
    gate_proj = project(rec_gate_weight)
    value_proj = project(value_weight).astype(jnp.bfloat16)
    rec_in = project(rec_in_weight).astype(jnp.bfloat16)
    queries = rms_scale(query_proj.reshape(seq_count, length, ATT_HEADS, HEAD_DIM), query_gain).astype(jnp.bfloat16)
    queries = queries.transpose(0, 2, 1, 3).reshape(seq_count, KV_HEADS, head_group, length, HEAD_DIM)
    key_heads = rms_scale(key_proj.reshape(seq_count, length, KV_HEADS, HEAD_DIM), key_gain).astype(jnp.bfloat16)
    key_heads = key_heads.transpose(0, 2, 1, 3)
    value_heads = value_proj.reshape(seq_count, length, KV_HEADS, HEAD_DIM).transpose(0, 2, 1, 3)
    blocks = attention(queries, key_heads, value_heads, forget_cache)
    attended = blocks.transpose(1, 0, 4, 2, 3, 5).reshape(row_count, ATT_HEADS, HEAD_DIM)
    att_normed = rms_scale(attended, attn_out_gain.reshape(ATT_HEADS, HEAD_DIM)).astype(jnp.bfloat16)
    att_normed = att_normed.reshape(row_count, ATT_WIDTH)
    rec_seq = rec_in.reshape(seq_count, length, LRU_WIDTH)
    padded = jnp.pad(rec_seq, ((0, 0), (CONV_TAPS - 1, 0), (0, 0)))
    conv = jnp.zeros((seq_count, length, LRU_WIDTH), jnp.float32)
    for tap in range(CONV_TAPS):
        conv = conv + padded[:, tap:tap + length].astype(jnp.float32) * conv_weight[tap].astype(jnp.float32)
    conv = conv.astype(jnp.bfloat16)
    conv_wide = conv.astype(jnp.float32)
    grouped = conv_wide.reshape(seq_count, length, LRU_BLOCKS, LRU_BLOCK)
    gate_decay = jnp.einsum('bsnd,nde->bsne', grouped, decay_gate_weight.astype(jnp.float32))
    gate_decay = gate_decay.reshape(seq_count, length, LRU_WIDTH)
    gate_input = jnp.einsum('bsnd,nde->bsne', grouped, input_gate_weight.astype(jnp.float32))
    gate_input = gate_input.reshape(seq_count, length, LRU_WIDTH)
    log_decay = -lru_const * jax.nn.sigmoid(gate_decay) * jax.nn.softplus(-decay_param) + decay_extra
    drive = jnp.sqrt(-jnp.expm1(2.0 * log_decay)) * jax.nn.sigmoid(gate_input) * conv_wide
    unused_decay, state = lax.associative_scan(merge_state, (jnp.exp(log_decay), drive), axis=1)
    gated = state * jax.nn.gelu(gate_proj.reshape(seq_count, length, LRU_WIDTH))
    rec_normed = rms_scale(gated.reshape(row_count, LRU_BLOCKS, LRU_BLOCK), rec_out_gain.reshape(LRU_BLOCKS, LRU_BLOCK)).astype(jnp.bfloat16)
    rec_normed = rec_normed.reshape(row_count, LRU_WIDTH)
    mixed = jnp.dot(att_normed, out_att_weight, preferred_element_type=jnp.float32)
    mixed = mixed + jnp.dot(rec_normed, out_rec_weight, preferred_element_type=jnp.float32)
    return mixed.astype(jnp.bfloat16).reshape(seq_count, length, model_width)
```

```python
import functools

import jax
import jax.numpy as jnp
from jax import lax
from jax.experimental import pallas as pl
from jax.experimental.pallas import tpu as pltpu
from jax.sharding import PartitionSpec as P

LRU_CONST = 8.0
EPS = 1e-06
F32 = jnp.float32
BF16 = jnp.bfloat16
MESH = pl.DeviceIdType.MESH


def group_rms(values, gain, width):
    parts = []
    for start in range(0, values.shape[1], width):
        part = values[:, start : start + width]
        scale = lax.rsqrt(jnp.mean(part * part, axis=-1, keepdims=True) + EPS)
        parts.append(part * scale)
    return jnp.concatenate(parts, axis=1) * gain


def one_minus_exp(y):
    series = y * (1 + y / 2 * (1 + y / 3 * (1 + y / 4 * (1 + y / 5 * (1 + y / 6 * (1 + y / 7))))))
    return -jnp.where(y > -0.4, series, jnp.exp(y) - 1.0)


def softplus(x):
    u = jnp.exp(-jnp.abs(x))
    s = u / (2.0 + u)
    q = s * s
    series = 1.0 / 17
    for odd in (15, 13, 11, 9, 7, 5, 3, 1):
        series = series * q + 1.0 / odd
    return jnp.maximum(x, 0.0) + 2.0 * s * series


def sigmoid(x):
    return 1.0 / (1.0 + jnp.exp(-x))


def gelu(x):
    return 0.5 * x * (1.0 + jnp.tanh(0.7978845608028654 * (x + 0.044715 * x * x * x)))


def dot(a, b):
    return jnp.dot(a, b, preferred_element_type=F32)


def kernel(
    dims,
    x_ref, norm_ref, wq_ref, wk_ref, wv_ref, qg_ref, kg_ref, fc_ref, wr_ref, wg_ref, cw_ref,
    dgw_ref, igw_ref, dp_ref, de_ref, ag_ref, rg_ref, oa_ref, or_ref,
    out_ref,
    xall, xsend, kvw, rw, qw, gw, kv_all, deg, rin, halo, st_all, act, halves, sums, parts, got,
    zs, zr, fs, fr, xas, xar, xbs, xbr, xcs, xcr, xds, xdr, des, der, kvs, kvr, hs, hr, ss, sr,
    acs, acr, ps, pr, qs, qr,
):
    n, nt, span, head_dim, flip = dims
    no, nto, ng = n // 2, nt // 2, n // 4
    me = lax.axis_index("sp")
    outer, inner = lax.div(me, 2), lax.rem(me, 2)
    grp, mem = lax.div(outer, 2), lax.rem(outer, 2)
    opp, omem = 1 - inner, 1 - mem
    mate = outer * 2 + opp
    pair = (grp * 2 + omem) * 2 + inner
    cross = (grp * 2 + omem) * 2 + opp
    tme = lax.axis_index("tp")
    touter, tinner = lax.div(tme, 2), lax.rem(tme, 2)
    tmate = touter * 2 + (1 - tinner)
    kr, channels = wq_ref.shape
    kvc = wk_ref.shape[0 if flip else 1]
    width = x_ref.shape[1]
    half = channels // 2
    quarter = width // nt
    heads = half // head_dim
    taps = cw_ref.shape[0]
    gp = 4 * span

    def rows_of(i, size):
        return pl.ds(pl.multiple_of(i * size, size), size)

    def to_outer(d):
        return lax.rem(outer + d, no)

    def from_outer(d):
        return lax.rem(outer + no - d, no)

    def copy(src, dst, send, recv, **where):
        return pltpu.make_async_remote_copy(
            src_ref=src, dst_ref=dst, send_sem=send, recv_sem=recv, device_id=where, device_id_type=MESH
        )

    barrier = pltpu.get_barrier_semaphore()
    for d in range(1, n):
        pl.semaphore_signal(barrier, inc=1, device_id={"sp": lax.rem(me + d, n)}, device_id_type=MESH)
    for d in range(1, nt):
        pl.semaphore_signal(barrier, inc=1, device_id={"tp": lax.rem(tme + d, nt)}, device_id_type=MESH)

    mine_block, mate_block = mem * 2 + inner, mem * 2 + opp
    pair_block, cross_block = omem * 2 + inner, omem * 2 + opp
    my_half, my_rows = rows_of(mem, half), rows_of(me, kr)
    my_cols = rows_of(tme, quarter)

    if flip:
        kvw[0:kvc, my_rows] = wk_ref[...]
        kvw[kvc : 2 * kvc, my_rows] = wv_ref[...]
    else:
        kvw[my_rows, :] = jnp.concatenate([wk_ref[...], wv_ref[...]], axis=1)

    def scale_rows(seq):
        x = x_ref[rows_of(seq, span), :].astype(F32)
        return lax.rsqrt(jnp.mean(x * x, axis=-1, keepdims=True) + EPS)

    xsend[...] = (
        x_ref[rows_of(opp, span), my_cols].astype(F32) * scale_rows(opp) * norm_ref[:, my_cols]
    ).astype(BF16)
    xall[mine_block] = (x_ref[rows_of(inner, span), :].astype(F32) * scale_rows(inner) * norm_ref[...]).astype(BF16)
    pl.semaphore_wait(barrier, n - 1 + nt - 1)

    weights = (None, wr_ref, wq_ref, wg_ref)
    buffers = (kvw, rw, qw, gw)

    def place(c, who):
        return kvw.at[:, rows_of(who, kr)] if c == 0 and flip else buffers[c].at[rows_of(who, kr), :]

    def origin(c, member):
        return place(0, me) if c == 0 else weights[c].at[:, rows_of(member, half)]

    def outward(c, d):
        to = to_outer(d)
        return copy(origin(c, lax.rem(to, 2)), place(c, me), zs.at[c, d - 1], zr.at[c, d - 1], sp=to * 2 + inner)

    def inward(c, d):
        who = from_outer(d) * 2 + inner
        return copy(place(c, who), place(c, who), zs.at[c, d - 1], zr.at[c, d - 1], sp=mate)

    def across(c, d, who, src=None):
        return copy(place(c, who) if src is None else src, place(c, who), fs.at[c, d], fr.at[c, d], sp=mate)

    def send_own(c):
        for d in range(1, no):
            outward(c, d).start()
        across(c, 0, me, origin(c, mem)).start()

    def forward(c):
        for d in range(1, no):
            inward(c, d).wait_recv()
            across(c, d, from_outer(d) * 2 + inner).start()

    def finish(c):
        for d in range(no):
            across(c, d, from_outer(d) * 2 + opp).wait_recv()

    def drain(c):
        for d in range(1, no):
            outward(c, d).wait_send()
        across(c, 0, me, origin(c, mem)).wait_send()
        for d in range(1, no):
            across(c, d, from_outer(d) * 2 + inner).wait_send()

    def piece_of(block, who=None):
        return xall.at[block, :, my_cols if who is None else rows_of(who, quarter)]

    to_mate_x = copy(xsend, piece_of(mine_block), xas, xar, sp=mate)
    to_pair_x = [
        copy(piece_of(mine_block), piece_of(mine_block), xbs.at[0], xbr.at[0], sp=pair),
        copy(piece_of(mate_block), piece_of(mate_block), xbs.at[1], xbr.at[1], sp=pair),
    ]
    shared = (mate_block, pair_block, cross_block)

    def to_far_x(k, d):
        far = lax.rem(touter + d, nto) * 2 + tinner
        return copy(piece_of(shared[k]), piece_of(shared[k]), xcs.at[k, d - 1], xcr.at[k, d - 1], tp=far)

    def to_core_x(k, d):
        ref = piece_of(shared[k], lax.rem(touter + nto - d, nto) * 2 + tinner)
        return copy(ref, ref, xds.at[k, d], xdr.at[k, d], tp=tmate)

    def spread(k):
        for d in range(1, nto):
            to_far_x(k, d).start()
        to_core_x(k, 0).start()

    def extra(i):
        to, seq, member = ((mate, opp, mem), (pair, inner, omem), (cross, opp, omem))[i]
        src = de_ref.at[rows_of(seq, span), rows_of(member, half)]
        return copy(src, deg.at[mine_block], des.at[i], der.at[i], sp=to)

    to_mate_x.start()
    to_pair_x[0].start()
    send_own(0)
    for i in range(3):
        extra(i).start()
    send_own(1)
    deg[mine_block] = de_ref[rows_of(inner, span), my_half]
    rw[my_rows, :] = wr_ref[:, my_half]
    qw[my_rows, :] = wq_ref[:, my_half]
    gw[my_rows, :] = wg_ref[:, my_half]

    to_mate_x.wait_recv()
    to_pair_x[1].start()
    spread(0)
    to_pair_x[0].wait_recv()
    spread(1)
    send_own(2)
    forward(0)
    to_pair_x[1].wait_recv()
    spread(2)
    send_own(3)
    for k in range(3):
        for d in range(1, nto):
            to_far_x(k, d).wait_recv()
            to_core_x(k, d).start()
    forward(1)
    for k in range(3):
        for d in range(nto):
            to_core_x(k, d).wait_recv()
    finish(0)

    def normed():
        return xall[...].reshape(gp, width)

    kv = lax.dot_general(normed(), kvw[...], (((1,), (1 if flip else 0,)), ((), ())), preferred_element_type=F32)
    keys = group_rms(kv[:, :kvc], kg_ref[...], head_dim)
    kv_all[grp] = jnp.concatenate([keys, kv[:, kvc:]], axis=1).astype(BF16)

    def kv_copy(d, who):
        to = lax.rem(grp + d, ng) * 4 + mem * 2 + inner
        return copy(kv_all.at[who], kv_all.at[who], kvs.at[d - 1], kvr.at[d - 1], sp=to)

    def state_copy(d, who):
        to = lax.rem(grp + d, ng) * 4 + mem * 2 + inner
        return copy(st_all.at[who], st_all.at[who], ss.at[d - 1], sr.at[d - 1], sp=to)

    def later(make, act_on):
        for d in range(1, ng):
            @pl.when(grp + d < ng)
            def _(d=d):
                act_on(make(d, grp))

    def earlier(make):
        for d in range(1, ng):
            @pl.when(grp >= d)
            def _(d=d):
                make(d, lax.rem(grp + ng - d, ng)).wait_recv()

    later(kv_copy, lambda c: c.start())

    finish(1)
    rec = dot(normed(), rw[...]).astype(BF16).astype(F32)
    rin[pl.ds(8, gp), :] = rec
    halo[0] = rec[gp - 8 : gp]
    halo[1] = jnp.zeros_like(halo[1])
    halo_copy = copy(halo.at[0], halo.at[2], hs, hr, sp=lax.rem(grp + 1, ng) * 4 + mem * 2 + inner)

    @pl.when(grp + 1 < ng)
    def _():
        halo_copy.start()

    forward(2)
    finish(2)
    scaling = head_dim ** (-0.5)
    query = dot(normed(), qw[...])
    queries = [
        (group_rms(query[:, h * head_dim : (h + 1) * head_dim], qg_ref[...], head_dim).astype(BF16) * scaling).astype(BF16)
        for h in range(heads)
    ]

    @pl.when(grp > 0)
    def _():
        halo_copy.wait_recv()
        halo[1] = halo[2]

    for i, block in ((0, mate_block), (1, pair_block), (2, cross_block)):
        copy(deg.at[block], deg.at[block], des.at[i], der.at[i], sp=mate).wait_recv()
    rin[pl.ds(0, 8), :] = halo[1]
    cw = cw_ref[:, my_half].astype(F32)
    conv = jnp.zeros((gp, half), F32)
    for tap in range(taps):
        conv = conv + rin[pl.ds(8 - (taps - 1) + tap, gp), :] * cw[tap : tap + 1]
    conv = conv.astype(BF16)
    lb = dgw_ref.shape[1]
    nb = half // lb
    gate_decay = jnp.concatenate([dot(conv[:, i * lb : (i + 1) * lb], dgw_ref[mem * nb + i]) for i in range(nb)], axis=1)
    gate_input = jnp.concatenate([dot(conv[:, i * lb : (i + 1) * lb], igw_ref[mem * nb + i]) for i in range(nb)], axis=1)
    log_decay = -LRU_CONST * sigmoid(gate_decay) * softplus(-dp_ref[:, my_half]) + deg[...].reshape(gp, half)
    state = jnp.sqrt(one_minus_exp(2.0 * log_decay)) * sigmoid(gate_input) * conv.astype(F32)
    decay = jnp.exp(log_decay)
    time = lax.broadcasted_iota(jnp.int32, state.shape, 0)
    shift = 1
    while shift < gp:
        if shift < 8:
            seen = time >= shift
            state = state + decay * jnp.where(seen, pltpu.roll(state, shift, 0), 0.0)
            decay = decay * jnp.where(seen, pltpu.roll(decay, shift, 0), 1.0)
        else:
            moved = state[shift:] + decay[shift:] * state[: gp - shift]
            faded = decay[shift:] * decay[: gp - shift]
            state = jnp.concatenate([state[:shift], moved], axis=0)
            decay = jnp.concatenate([decay[:shift], faded], axis=0)
        shift *= 2
    st_all[grp, pl.ds(0, 1), :] = decay[gp - 1 : gp]
    st_all[grp, pl.ds(1, 1), :] = state[gp - 1 : gp]
    later(state_copy, lambda c: c.start())

    def attend(carried, q, kb, vb, fade_row, mask):
        top, total, accum = carried
        s = lax.dot_general(q, kb, (((1,), (1,)), ((), ())), preferred_element_type=F32) - fade_row
        if mask is not None:
            s = jnp.where(mask, s, -jnp.inf)
        new_top = jnp.maximum(top, jnp.max(s, axis=-1, keepdims=True))
        w = jnp.exp(s - new_top)
        fade = jnp.exp(top - new_top)
        total = total * fade + jnp.sum(w, axis=-1, keepdims=True)
        return new_top, total, accum * fade + dot(w.astype(BF16), vb)

    qb = gp // 2
    jobs = [(h, i) for h in range(heads) for i in range(2)]
    kv_own = kv_all[grp]
    carried = []
    for h, i in jobs:
        size = (i + 1) * qb
        kb, vb = kv_own[:size, :kvc], kv_own[:size, kvc:]
        fade_row = fc_ref[inner, pl.ds(mem * heads + h, 1), pl.ds(pl.multiple_of(grp * gp, gp), size)]
        mask = i * qb + lax.broadcasted_iota(jnp.int32, (qb, size), 0) >= lax.broadcasted_iota(jnp.int32, (qb, size), 1)
        start = (jnp.full((qb, 1), -1e30, F32), jnp.zeros((qb, 1), F32), jnp.zeros((qb, head_dim), F32))
        carried.append(attend(start, queries[h][i * qb : size], kb, vb, fade_row, mask))

    forward(3)
    earlier(kv_copy)

    def step(j, carried):
        result = []
        kb, vb = kv_all[j, :, :kvc], kv_all[j, :, kvc:]
        for (h, i), state_of in zip(jobs, carried):
            fade_row = fc_ref[inner, pl.ds(mem * heads + h, 1), pl.ds(pl.multiple_of(j * gp, gp), gp)]
            result.append(attend(state_of, queries[h][i * qb : (i + 1) * qb], kb, vb, fade_row, None))
        return tuple(result)

    carried = lax.fori_loop(0, grp, step, tuple(carried))
    columns = []
    for h in range(heads):
        pieces = []
        for (hh, i), (top, total, accum) in zip(jobs, carried):
            if hh == h:
                value = accum / total
                pieces.append(value * lax.rsqrt(jnp.mean(value * value, axis=-1, keepdims=True) + EPS))
        columns.append(jnp.concatenate(pieces, axis=0))

    def act_copy(a, i):
        to, block = ((mate, mate_block), (pair, pair_block), (cross, cross_block))[i]
        return copy(
            act.at[a, block], halves.at[a, rows_of(inner, span), my_half], acs.at[a, i], acr.at[a, i], sp=to
        )

    def act_from(a, i):
        seq, member = ((opp, mem), (inner, omem), (opp, omem))[i]
        ref = halves.at[a, rows_of(seq, span), rows_of(member, half)]
        return copy(ref, ref, acs.at[a, i], acr.at[a, i], sp=mate)

    def hand_out(a, values):
        act[a] = values.astype(BF16).reshape(4, span, half)
        for i in range(3):
            act_copy(a, i).start()
        halves[a, rows_of(inner, span), my_half] = act[a, mine_block]

    hand_out(0, jnp.concatenate(columns, axis=1) * ag_ref[:, my_half])

    earlier(state_copy)

    def enter(j, e):
        return st_all[j, pl.ds(0, 1), :] * e + st_all[j, pl.ds(1, 1), :]

    entering = lax.fori_loop(0, grp, enter, jnp.zeros((1, half), F32))
    whole_state = state + decay * entering
    finish(3)
    gated = whole_state * gelu(dot(normed(), gw[...]))
    hand_out(1, group_rms(gated, rg_ref[:, my_half], lb))
    for a in range(2):
        for i in range(3):
            act_from(a, i).wait_recv()

    cols = out_ref.shape[1]

    def piece(who):
        span_cols = pl.ds(pl.multiple_of(who * cols, cols), cols)
        return dot(halves[0], oa_ref[:, span_cols]) + dot(halves[1], or_ref[:, span_cols])

    def to_mate(s):
        return pltpu.make_async_remote_copy(
            src_ref=sums.at[s], dst_ref=parts.at[s], send_sem=ps.at[s], recv_sem=pr.at[s],
            device_id={"tp": tmate}, device_id_type=MESH,
        )

    def to_far(d):
        return pltpu.make_async_remote_copy(
            src_ref=sums.at[nto + d - 1], dst_ref=got.at[d - 1], send_sem=qs.at[d - 1], recv_sem=qr.at[d - 1],
            device_id={"tp": lax.rem(touter + d, nto) * 2 + tinner}, device_id_type=MESH,
        )

    for s in list(range(1, nto)) + [0]:
        sums[s] = piece(lax.rem(touter + s, nto) * 2 + (1 - tinner)).astype(BF16)
        to_mate(s).start()
    for d in range(1, nto):
        mine = piece(lax.rem(touter + d, nto) * 2 + tinner)
        to_mate(d).wait_recv()
        sums[nto + d - 1] = (mine + parts[d].astype(F32)).astype(BF16)
        to_far(d).start()
    mine = piece(tme)
    to_mate(0).wait_recv()
    mine = mine + parts[0].astype(F32)
    for d in range(1, nto):
        to_far(d).wait_recv()
        mine = mine + got[d - 1].astype(F32)
    out_ref[...] = mine.astype(BF16)

    for c in range(4):
        drain(c)
    to_mate_x.wait_send()
    for c in to_pair_x:
        c.wait_send()
    for k in range(3):
        extra(k).wait_send()
        for d in range(1, nto):
            to_far_x(k, d).wait_send()
        for d in range(nto):
            to_core_x(k, d).wait_send()
    later(kv_copy, lambda c: c.wait_send())
    later(state_copy, lambda c: c.wait_send())

    @pl.when(grp + 1 < ng)
    def _():
        halo_copy.wait_send()

    for a in range(2):
        for i in range(3):
            act_copy(a, i).wait_send()
    for s in range(nto):
        to_mate(s).wait_send()
    for d in range(1, nto):
        to_far(d).wait_send()


def body(
    n, nt,
    inputs, norm_gain, query_weight, key_weight, value_weight, query_gain, key_gain, forget_cache,
    rec_in_weight, rec_gate_weight, conv_weight, decay_gate_weight, input_gate_weight, decay_param,
    decay_extra, attn_out_gain, rec_out_gain, out_att_weight, out_rec_weight,
):
    seqs, span, width = inputs.shape
    assert seqs == 2 and n % 4 == 0 and nt % 2 == 0 and key_weight.shape[1] == query_gain.shape[0]
    rows = seqs * span
    head_dim = query_gain.shape[0]
    channels = rec_in_weight.shape[1]
    qc, kvc = query_weight.shape[1], key_weight.shape[1]
    half = channels // 2
    cols = out_att_weight.shape[1] // nt
    flip = query_weight.shape[0] % 128 == 0
    kv_weights = [w.T if flip else w for w in (key_weight, value_weight)]
    no, nto, ng = n // 2, nt // 2, n // 4
    dma = pltpu.SemaphoreType.DMA
    vmem = pl.BlockSpec(memory_space=pltpu.VMEM)
    out = pl.pallas_call(
        functools.partial(kernel, (n, nt, span, head_dim, flip)),
        out_shape=jax.ShapeDtypeStruct((rows, cols), BF16),
        in_specs=[vmem] * 19,
        out_specs=vmem,
        scratch_shapes=[
            pltpu.VMEM((4, span, width), BF16),
            pltpu.VMEM((span, width // nt), BF16),
            pltpu.VMEM((2 * kvc, width) if flip else (width, 2 * kvc), BF16),
            pltpu.VMEM((width, half), BF16),
            pltpu.VMEM((width, half), BF16),
            pltpu.VMEM((width, half), BF16),
            pltpu.VMEM((ng, 4 * span, 2 * kvc), BF16),
            pltpu.VMEM((4, span, half), F32),
            pltpu.VMEM((4 * span + 8, half), F32),
            pltpu.VMEM((3, 8, half), F32),
            pltpu.VMEM((ng, 8, half), F32),
            pltpu.VMEM((2, 4, span, half), BF16),
            pltpu.VMEM((2, rows, channels), BF16),
            pltpu.VMEM((2 * nto, rows, cols), BF16),
            pltpu.VMEM((nto, rows, cols), BF16),
            pltpu.VMEM((nto, rows, cols), BF16),
            dma((4, no)), dma((4, no)), dma((4, no)), dma((4, no)),
            dma, dma, dma((2,)), dma((2,)), dma((3, nto)), dma((3, nto)), dma((3, nto)), dma((3, nto)),
            dma((3,)), dma((3,)), dma((ng,)), dma((ng,)), dma, dma, dma((ng,)), dma((ng,)),
            dma((2, 3)), dma((2, 3)), dma((nto,)), dma((nto,)), dma((nto,)), dma((nto,)),
        ],
        compiler_params=pltpu.CompilerParams(
            collective_id=0, has_side_effects=True, vmem_limit_bytes=60 * 1024 * 1024
        ),
    )(
        inputs.reshape(rows, width), norm_gain.reshape(1, width), query_weight, *kv_weights,
        query_gain.reshape(1, head_dim), key_gain.reshape(1, head_dim), forget_cache,
        rec_in_weight, rec_gate_weight, conv_weight, decay_gate_weight, input_gate_weight,
        decay_param.reshape(1, channels), decay_extra.reshape(rows, channels),
        attn_out_gain.reshape(1, qc), rec_out_gain.reshape(1, channels), out_att_weight, out_rec_weight,
    )
    return out.reshape(seqs, span, cols)


def solution(mesh):
    return jax.shard_map(
        functools.partial(body, mesh.shape["sp"], mesh.shape["tp"]),
        mesh=mesh,
        in_specs=(
            P(None, "sp", None), P(), P("sp", "tp"), P("sp", "tp"), P("sp", "tp"), P(), P(),
            P(None, "tp", None), P("sp", "tp"), P("sp", "tp"), P(None, "tp"), P("tp", None, None),
            P("tp", None, None), P("tp"), P(None, "sp", "tp"), P("tp"), P("tp"), P("tp", None), P("tp", None),
        ),
        out_specs=P(None, "sp", "tp"),
        check_vma=False,
    )
```

```python
import functools

import jax
import jax.numpy as jnp
from jax import lax
from jax.experimental import pallas as pl
from jax.experimental.pallas import tpu as pltpu
from jax.sharding import PartitionSpec as P

LRU_CONST = 8.0
EPS = 1e-06
F32 = jnp.float32
BF16 = jnp.bfloat16
MESH = pl.DeviceIdType.MESH


def group_rms(values, gain, width):
    parts = []
    for start in range(0, values.shape[1], width):
        part = values[:, start : start + width]
        scale = lax.rsqrt(jnp.mean(part * part, axis=-1, keepdims=True) + EPS)
        parts.append(part * scale)
    return jnp.concatenate(parts, axis=1) * gain


def one_minus_exp(y):
    series = y * (1 + y / 2 * (1 + y / 3 * (1 + y / 4 * (1 + y / 5 * (1 + y / 6 * (1 + y / 7))))))
    return -jnp.where(y > -0.4, series, jnp.exp(y) - 1.0)


def softplus(x):
    u = jnp.exp(-jnp.abs(x))
    s = u / (2.0 + u)
    q = s * s
    series = 1.0 / 17
    for odd in (15, 13, 11, 9, 7, 5, 3, 1):
        series = series * q + 1.0 / odd
    return jnp.maximum(x, 0.0) + 2.0 * s * series


def sigmoid(x):
    return 1.0 / (1.0 + jnp.exp(-x))


def gelu(x):
    return 0.5 * x * (1.0 + jnp.tanh(0.7978845608028654 * (x + 0.044715 * x * x * x)))


def dot(a, b):
    return jnp.dot(a, b, preferred_element_type=F32)


def kernel(
    dims,
    x_ref, norm_ref, wq_ref, wk_ref, wv_ref, qg_ref, kg_ref, fc_ref, wr_ref, wg_ref, cw_ref,
    dgw_ref, igw_ref, dp_ref, de_ref, ag_ref, rg_ref, oa_ref, or_ref,
    out_ref,
    xall, xsend, kvsrc, kvw, rw, qw, gw, kv_all, scanned, deg, rin, halo, st_all, act, halves, sums, parts, got,
    zs, zr, fs, fr, xas, xar, xbs, xbr, xcs, xcr, xds, xdr, des, der, kvs, kvr, kps, kpr, hs, hr, ss, sr,
    acs, acr, ps, pr, qs, qr,
):
    n, nt, span, head_dim, flip = dims
    no, nto, ng = n // 2, nt // 2, n // 4
    me = lax.axis_index("sp")
    outer, inner = lax.div(me, 2), lax.rem(me, 2)
    grp, mem = lax.div(outer, 2), lax.rem(outer, 2)
    opp, omem = 1 - inner, 1 - mem
    mate = outer * 2 + opp
    pair = (grp * 2 + omem) * 2 + inner
    cross = (grp * 2 + omem) * 2 + opp
    tme = lax.axis_index("tp")
    touter, tinner = lax.div(tme, 2), lax.rem(tme, 2)
    tmate = touter * 2 + (1 - tinner)
    kr, channels = wq_ref.shape
    kvc = wk_ref.shape[0 if flip else 1]
    width = x_ref.shape[1]
    half = channels // 2
    quarter = width // nt
    heads = half // head_dim
    taps = cw_ref.shape[0]
    gp = 4 * span

    def rows_of(i, size):
        return pl.ds(pl.multiple_of(i * size, size), size)

    def partner(d):
        who, bit = 0, 1
        while bit < no:
            own = lax.rem(lax.div(outer, bit), 2)
            who = who + bit * (1 - own if d & bit else own)
            bit *= 2
        return who

    def copy(src, dst, send, recv, **where):
        return pltpu.make_async_remote_copy(
            src_ref=src, dst_ref=dst, send_sem=send, recv_sem=recv, device_id=where, device_id_type=MESH
        )

    barrier = pltpu.get_barrier_semaphore()
    for d in range(1, n):
        pl.semaphore_signal(barrier, inc=1, device_id={"sp": lax.rem(me + d, n)}, device_id_type=MESH)
    for d in range(1, nt):
        pl.semaphore_signal(barrier, inc=1, device_id={"tp": lax.rem(tme + d, nt)}, device_id_type=MESH)

    mine_block, mate_block = mem * 2 + inner, mem * 2 + opp
    pair_block, cross_block = omem * 2 + inner, omem * 2 + opp
    my_half, my_rows = rows_of(mem, half), rows_of(me, kr)
    my_cols = rows_of(tme, quarter)

    kvsrc[0] = wk_ref[...]
    kvsrc[1] = wv_ref[...]

    def scale_rows(seq):
        x = x_ref[rows_of(seq, span), :].astype(F32)
        return lax.rsqrt(jnp.mean(x * x, axis=-1, keepdims=True) + EPS)

    xsend[...] = (
        x_ref[rows_of(opp, span), my_cols].astype(F32) * scale_rows(opp) * norm_ref[:, my_cols]
    ).astype(BF16)
    xall[mine_block] = (x_ref[rows_of(inner, span), :].astype(F32) * scale_rows(inner) * norm_ref[...]).astype(BF16)
    pl.semaphore_wait(barrier, n - 1 + nt - 1)

    weights = (None, wr_ref, wq_ref, wg_ref)
    buffers = (kvw, rw, qw, gw)

    def place(c, who):
        return kvw.at[:, rows_of(who, kr)] if c == 0 and flip else buffers[c].at[rows_of(who, kr), :]

    def origin(c, member):
        return kvsrc.at[member] if c == 0 else weights[c].at[:, rows_of(member, half)]

    def outward(c, d):
        to = partner(d)
        return copy(origin(c, lax.rem(to, 2)), place(c, me), zs.at[c, d - 1], zr.at[c, d - 1], sp=to * 2 + inner)

    def inward(c, d):
        who = partner(d) * 2 + inner
        return copy(place(c, who), place(c, who), zs.at[c, d - 1], zr.at[c, d - 1], sp=mate)

    def across(c, d, who, src=None):
        return copy(place(c, who) if src is None else src, place(c, who), fs.at[c, d], fr.at[c, d], sp=mate)

    def send_z(c):
        for d in range(1, no):
            outward(c, d).start()

    def send_y(c):
        across(c, 0, me, origin(c, mem)).start()

    def forward(c, which=range(1, no)):
        for d in which:
            inward(c, d).wait_recv()
            across(c, d, partner(d) * 2 + inner).start()

    def finish(c):
        for d in range(no):
            across(c, d, partner(d) * 2 + opp).wait_recv()

    def drain(c):
        for d in range(1, no):
            outward(c, d).wait_send()
        across(c, 0, me, origin(c, mem)).wait_send()
        for d in range(1, no):
            across(c, d, partner(d) * 2 + inner).wait_send()

    def piece_of(block, who=None):
        return xall.at[block, :, my_cols if who is None else rows_of(who, quarter)]

    to_mate_x = copy(xsend, piece_of(mine_block), xas, xar, sp=mate)
    to_pair_x = [
        copy(piece_of(mine_block), piece_of(mine_block), xbs.at[0], xbr.at[0], sp=pair),
        copy(piece_of(mate_block), piece_of(mate_block), xbs.at[1], xbr.at[1], sp=pair),
    ]
    shared = (mate_block, pair_block, cross_block)

    def to_far_x(k, d):
        far = lax.rem(touter + d, nto) * 2 + tinner
        return copy(piece_of(shared[k]), piece_of(shared[k]), xcs.at[k, d - 1], xcr.at[k, d - 1], tp=far)

    def to_core_x(k, d):
        ref = piece_of(shared[k], lax.rem(touter + nto - d, nto) * 2 + tinner)
        return copy(ref, ref, xds.at[k, d], xdr.at[k, d], tp=tmate)

    def spread(k):
        for d in range(1, nto):
            to_far_x(k, d).start()
        to_core_x(k, 0).start()

    def extra(i):
        to, seq, member = ((mate, opp, mem), (pair, inner, omem), (cross, opp, omem))[i]
        src = de_ref.at[rows_of(seq, span), rows_of(member, half)]
        return copy(src, deg.at[mine_block], des.at[i], der.at[i], sp=to)

    to_mate_x.start()
    to_pair_x[0].start()
    send_z(0)
    for c in range(3):
        send_y(c)
    deg[mine_block] = de_ref[rows_of(inner, span), my_half]
    if flip:
        kvw[:, my_rows] = kvsrc[mem]
    else:
        kvw[my_rows, :] = kvsrc[mem]
    rw[my_rows, :] = wr_ref[:, my_half]
    qw[my_rows, :] = wq_ref[:, my_half]
    gw[my_rows, :] = wg_ref[:, my_half]

    to_mate_x.wait_recv()
    to_pair_x[1].start()
    spread(0)
    send_z(1)
    to_pair_x[0].wait_recv()
    spread(1)
    forward(0)
    send_y(3)
    to_pair_x[1].wait_recv()
    spread(2)
    send_z(2)
    for i in range(3):
        extra(i).start()
    forward(1)
    for k in range(3):
        for d in range(1, nto):
            to_far_x(k, d).wait_recv()
            to_core_x(k, d).start()
    for k in range(3):
        for d in range(nto):
            to_core_x(k, d).wait_recv()
    finish(0)

    def normed():
        return xall[...].reshape(gp, width)

    kv = lax.dot_general(normed(), kvw[...], (((1,), (1 if flip else 0,)), ((), ())), preferred_element_type=F32)
    kv = jnp.where(mem == 0, group_rms(kv, kg_ref[...], head_dim), kv).astype(BF16)
    kv_all[mem, grp] = jnp.concatenate([kv[: gp // 2], kv[gp // 2 :]], axis=1)

    def kv_copy(d, who):
        to, ref = lax.rem(grp + d, ng) * 4 + mem * 2 + inner, kv_all.at[mem, who]
        return copy(ref, ref, kvs.at[d - 1], kvr.at[d - 1], sp=to)

    def kv_pair(d, member, who):
        ref = kv_all.at[member, who]
        return copy(ref, ref, kps.at[d], kpr.at[d], sp=pair)

    def state_copy(d, who):
        to = lax.rem(grp + d, ng) * 4 + mem * 2 + inner
        return copy(st_all.at[who], st_all.at[who], ss.at[d - 1], sr.at[d - 1], sp=to)

    def later(make, act_on):
        for d in range(1, ng):
            @pl.when(grp + d < ng)
            def _(d=d):
                act_on(make(d, grp))

    def earlier(make):
        for d in range(1, ng):
            @pl.when(grp >= d)
            def _(d=d):
                make(d, lax.rem(grp + ng - d, ng)).wait_recv()

    kv_pair(0, mem, grp).start()
    later(kv_copy, lambda c: c.start())

    finish(1)
    rec = dot(normed(), rw[...]).astype(BF16).astype(F32)
    rin[pl.ds(8, gp), :] = rec
    halo[0] = rec[gp - 8 : gp]
    halo[1] = jnp.zeros_like(halo[1])
    halo_copy = copy(halo.at[0], halo.at[2], hs, hr, sp=lax.rem(grp + 1, ng) * 4 + mem * 2 + inner)

    @pl.when(grp + 1 < ng)
    def _():
        halo_copy.start()

    send_z(3)
    forward(2)
    lb = dgw_ref.shape[1]

    def recur():
        for i, block in ((0, mate_block), (1, pair_block), (2, cross_block)):
            copy(deg.at[block], deg.at[block], des.at[i], der.at[i], sp=mate).wait_recv()
        rin[pl.ds(0, 8), :] = halo[1]
        cw = cw_ref[:, my_half].astype(F32)
        conv = jnp.zeros((gp, half), F32)
        for tap in range(taps):
            conv = conv + rin[pl.ds(8 - (taps - 1) + tap, gp), :] * cw[tap : tap + 1]
        conv = conv.astype(BF16)
        nb = half // lb
        gate_decay = jnp.concatenate([dot(conv[:, i * lb : (i + 1) * lb], dgw_ref[mem * nb + i]) for i in range(nb)], axis=1)
        gate_input = jnp.concatenate([dot(conv[:, i * lb : (i + 1) * lb], igw_ref[mem * nb + i]) for i in range(nb)], axis=1)
        log_decay = -LRU_CONST * sigmoid(gate_decay) * softplus(-dp_ref[:, my_half]) + deg[...].reshape(gp, half)
        state = jnp.sqrt(one_minus_exp(2.0 * log_decay)) * sigmoid(gate_input) * conv.astype(F32)
        decay = jnp.exp(log_decay)
        time = lax.broadcasted_iota(jnp.int32, state.shape, 0)
        shift = 1
        while shift < gp:
            if shift < 8:
                seen = time >= shift
                state = state + decay * jnp.where(seen, pltpu.roll(state, shift, 0), 0.0)
                decay = decay * jnp.where(seen, pltpu.roll(decay, shift, 0), 1.0)
            else:
                moved = state[shift:] + decay[shift:] * state[: gp - shift]
                faded = decay[shift:] * decay[: gp - shift]
                state = jnp.concatenate([state[:shift], moved], axis=0)
                decay = jnp.concatenate([decay[:shift], faded], axis=0)
            shift *= 2
        scanned[0] = decay
        scanned[1] = state
        st_all[grp, pl.ds(0, 1), :] = decay[gp - 1 : gp]
        st_all[grp, pl.ds(1, 1), :] = state[gp - 1 : gp]
        later(state_copy, lambda c: c.start())

    @pl.when(grp == 0)
    def _():
        recur()

    finish(2)
    scaling = head_dim ** (-0.5)
    query = dot(normed(), qw[...])
    queries = [
        (group_rms(query[:, h * head_dim : (h + 1) * head_dim], qg_ref[...], head_dim).astype(BF16) * scaling).astype(BF16)
        for h in range(heads)
    ]

    forward(3, range(1, no - 1))
    kv_pair(0, omem, grp).wait_recv()
    def attend(carried, q, kb, vb, fade_row, mask):
        top, total, accum = carried
        s = lax.dot_general(q, kb, (((1,), (1,)), ((), ())), preferred_element_type=F32) - fade_row
        if mask is not None:
            s = jnp.where(mask, s, -jnp.inf)
        new_top = jnp.maximum(top, jnp.max(s, axis=-1, keepdims=True))
        w = jnp.exp(s - new_top)
        fade = jnp.exp(top - new_top)
        total = total * fade + jnp.sum(w, axis=-1, keepdims=True)
        return new_top, total, accum * fade + dot(w.astype(BF16), vb)

    qb = gp // 2
    jobs = [(h, i) for h in range(heads) for i in range(2)]

    def heads_of(which, j):
        packed = kv_all[which, j]
        return jnp.concatenate([packed[:, :kvc], packed[:, kvc:]], axis=0)

    k_own, v_own = heads_of(0, grp), heads_of(1, grp)
    carried = []
    for h, i in jobs:
        size = (i + 1) * qb
        kb, vb = k_own[:size], v_own[:size]
        fade_row = fc_ref[inner, pl.ds(mem * heads + h, 1), pl.ds(pl.multiple_of(grp * gp, gp), size)]
        mask = i * qb + lax.broadcasted_iota(jnp.int32, (qb, size), 0) >= lax.broadcasted_iota(jnp.int32, (qb, size), 1)
        start = (jnp.full((qb, 1), -1e30, F32), jnp.zeros((qb, 1), F32), jnp.zeros((qb, head_dim), F32))
        carried.append(attend(start, queries[h][i * qb : size], kb, vb, fade_row, mask))

    forward(3, range(no - 1, no))
    for d in range(1, ng):
        @pl.when(grp >= d)
        def _(d=d):
            who = lax.rem(grp + ng - d, ng)
            kv_copy(d, who).wait_recv()
            kv_pair(d, mem, who).start()

    for d in range(1, ng):
        @pl.when(grp >= d)
        def _(d=d):
            kv_pair(d, omem, lax.rem(grp + ng - d, ng)).wait_recv()


    def step(j, carried):
        result = []
        kb, vb = heads_of(0, j), heads_of(1, j)
        for (h, i), state_of in zip(jobs, carried):
            fade_row = fc_ref[inner, pl.ds(mem * heads + h, 1), pl.ds(pl.multiple_of(j * gp, gp), gp)]
            result.append(attend(state_of, queries[h][i * qb : (i + 1) * qb], kb, vb, fade_row, None))
        return tuple(result)

    carried = lax.fori_loop(0, grp, step, tuple(carried))
    columns = []
    for h in range(heads):
        pieces = []
        for (hh, i), (top, total, accum) in zip(jobs, carried):
            if hh == h:
                value = accum / total
                pieces.append(value * lax.rsqrt(jnp.mean(value * value, axis=-1, keepdims=True) + EPS))
        columns.append(jnp.concatenate(pieces, axis=0))

    def act_copy(a, i):
        to, block = ((mate, mate_block), (pair, pair_block), (cross, cross_block))[i]
        return copy(
            act.at[a, block], halves.at[a, rows_of(inner, span), my_half], acs.at[a, i], acr.at[a, i], sp=to
        )

    def act_from(a, i):
        seq, member = ((opp, mem), (inner, omem), (opp, omem))[i]
        ref = halves.at[a, rows_of(seq, span), rows_of(member, half)]
        return copy(ref, ref, acs.at[a, i], acr.at[a, i], sp=mate)

    def hand_out(a, values):
        act[a] = values.astype(BF16).reshape(4, span, half)
        for i in range(3):
            act_copy(a, i).start()
        halves[a, rows_of(inner, span), my_half] = act[a, mine_block]

    hand_out(0, jnp.concatenate(columns, axis=1) * ag_ref[:, my_half])

    @pl.when(grp > 0)
    def _():
        halo_copy.wait_recv()
        halo[1] = halo[2]
        recur()

    earlier(state_copy)

    def enter(j, e):
        return st_all[j, pl.ds(0, 1), :] * e + st_all[j, pl.ds(1, 1), :]

    entering = lax.fori_loop(0, grp, enter, jnp.zeros((1, half), F32))
    whole_state = scanned[1] + scanned[0] * entering
    finish(3)
    gated = whole_state * gelu(dot(normed(), gw[...]))
    hand_out(1, group_rms(gated, rg_ref[:, my_half], lb))
    for a in range(2):
        for i in range(3):
            act_from(a, i).wait_recv()

    cols = out_ref.shape[1]

    def piece(who):
        span_cols = pl.ds(pl.multiple_of(who * cols, cols), cols)
        return dot(halves[0], oa_ref[:, span_cols]) + dot(halves[1], or_ref[:, span_cols])

    def to_mate(s):
        return pltpu.make_async_remote_copy(
            src_ref=sums.at[s], dst_ref=parts.at[s], send_sem=ps.at[s], recv_sem=pr.at[s],
            device_id={"tp": tmate}, device_id_type=MESH,
        )

    def to_far(d):
        return pltpu.make_async_remote_copy(
            src_ref=sums.at[nto + d - 1], dst_ref=got.at[d - 1], send_sem=qs.at[d - 1], recv_sem=qr.at[d - 1],
            device_id={"tp": lax.rem(touter + d, nto) * 2 + tinner}, device_id_type=MESH,
        )

    for s in list(range(1, nto)) + [0]:
        sums[s] = piece(lax.rem(touter + s, nto) * 2 + (1 - tinner)).astype(BF16)
        to_mate(s).start()
    for d in range(1, nto):
        mine = piece(lax.rem(touter + d, nto) * 2 + tinner)
        to_mate(d).wait_recv()
        sums[nto + d - 1] = (mine + parts[d].astype(F32)).astype(BF16)
        to_far(d).start()
    mine = piece(tme)
    to_mate(0).wait_recv()
    mine = mine + parts[0].astype(F32)
    for d in range(1, nto):
        to_far(d).wait_recv()
        mine = mine + got[d - 1].astype(F32)
    out_ref[...] = mine.astype(BF16)

    for c in range(4):
        drain(c)
    to_mate_x.wait_send()
    for c in to_pair_x:
        c.wait_send()
    for k in range(3):
        extra(k).wait_send()
        for d in range(1, nto):
            to_far_x(k, d).wait_send()
        for d in range(nto):
            to_core_x(k, d).wait_send()
    later(kv_copy, lambda c: c.wait_send())
    kv_pair(0, mem, grp).wait_send()
    for d in range(1, ng):
        @pl.when(grp >= d)
        def _(d=d):
            kv_pair(d, mem, lax.rem(grp + ng - d, ng)).wait_send()

    later(state_copy, lambda c: c.wait_send())

    @pl.when(grp + 1 < ng)
    def _():
        halo_copy.wait_send()

    for a in range(2):
        for i in range(3):
            act_copy(a, i).wait_send()
    for s in range(nto):
        to_mate(s).wait_send()
    for d in range(1, nto):
        to_far(d).wait_send()


def body(
    n, nt,
    inputs, norm_gain, query_weight, key_weight, value_weight, query_gain, key_gain, forget_cache,
    rec_in_weight, rec_gate_weight, conv_weight, decay_gate_weight, input_gate_weight, decay_param,
    decay_extra, attn_out_gain, rec_out_gain, out_att_weight, out_rec_weight,
):
    seqs, span, width = inputs.shape
    assert seqs == 2 and n % 4 == 0 and nt % 2 == 0 and key_weight.shape[1] == query_gain.shape[0]
    rows = seqs * span
    head_dim = query_gain.shape[0]
    channels = rec_in_weight.shape[1]
    qc, kvc = query_weight.shape[1], key_weight.shape[1]
    half = channels // 2
    cols = out_att_weight.shape[1] // nt
    flip = query_weight.shape[0] % 128 == 0
    kv_weights = [w.T if flip else w for w in (key_weight, value_weight)]
    no, nto, ng = n // 2, nt // 2, n // 4
    dma = pltpu.SemaphoreType.DMA
    vmem = pl.BlockSpec(memory_space=pltpu.VMEM)
    out = pl.pallas_call(
        functools.partial(kernel, (n, nt, span, head_dim, flip)),
        out_shape=jax.ShapeDtypeStruct((rows, cols), BF16),
        in_specs=[vmem] * 19,
        out_specs=vmem,
        scratch_shapes=[
            pltpu.VMEM((4, span, width), BF16),
            pltpu.VMEM((span, width // nt), BF16),
            pltpu.VMEM((2, *kv_weights[0].shape), BF16),
            pltpu.VMEM((kvc, width) if flip else (width, kvc), BF16),
            pltpu.VMEM((width, half), BF16),
            pltpu.VMEM((width, half), BF16),
            pltpu.VMEM((width, half), BF16),
            pltpu.VMEM((2, ng, 2 * span, 2 * kvc), BF16),
            pltpu.VMEM((2, 4 * span, half), F32),
            pltpu.VMEM((4, span, half), F32),
            pltpu.VMEM((4 * span + 8, half), F32),
            pltpu.VMEM((3, 8, half), F32),
            pltpu.VMEM((ng, 8, half), F32),
            pltpu.VMEM((2, 4, span, half), BF16),
            pltpu.VMEM((2, rows, channels), BF16),
            pltpu.VMEM((2 * nto, rows, cols), BF16),
            pltpu.VMEM((nto, rows, cols), BF16),
            pltpu.VMEM((nto, rows, cols), BF16),
            dma((4, no)), dma((4, no)), dma((4, no)), dma((4, no)),
            dma, dma, dma((2,)), dma((2,)), dma((3, nto)), dma((3, nto)), dma((3, nto)), dma((3, nto)),
            dma((3,)), dma((3,)), dma((ng,)), dma((ng,)), dma((ng,)), dma((ng,)), dma, dma, dma((ng,)), dma((ng,)),
            dma((2, 3)), dma((2, 3)), dma((nto,)), dma((nto,)), dma((nto,)), dma((nto,)),
        ],
        compiler_params=pltpu.CompilerParams(
            collective_id=0, has_side_effects=True, vmem_limit_bytes=60 * 1024 * 1024
        ),
    )(
        inputs.reshape(rows, width), norm_gain.reshape(1, width), query_weight, *kv_weights,
        query_gain.reshape(1, head_dim), key_gain.reshape(1, head_dim), forget_cache,
        rec_in_weight, rec_gate_weight, conv_weight, decay_gate_weight, input_gate_weight,
        decay_param.reshape(1, channels), decay_extra.reshape(rows, channels),
        attn_out_gain.reshape(1, qc), rec_out_gain.reshape(1, channels), out_att_weight, out_rec_weight,
    )
    return out.reshape(seqs, span, cols)


def solution(mesh):
    return jax.shard_map(
        functools.partial(body, mesh.shape["sp"], mesh.shape["tp"]),
        mesh=mesh,
        in_specs=(
            P(None, "sp", None), P(), P("sp", "tp"), P("sp", "tp"), P("sp", "tp"), P(), P(),
            P(None, "tp", None), P("sp", "tp"), P("sp", "tp"), P(None, "tp"), P("tp", None, None),
            P("tp", None, None), P("tp"), P(None, "sp", "tp"), P("tp"), P("tp"), P("tp", None), P("tp", None),
        ),
        out_specs=P(None, "sp", "tp"),
        check_vma=False,
    )
```

```python
import functools

import jax
import jax.numpy as jnp
from jax import lax
from jax.experimental import pallas as pl
from jax.experimental.pallas import tpu as pltpu
from jax.sharding import PartitionSpec as P

LRU_CONST = 8.0
EPS = 1e-06
F32 = jnp.float32
BF16 = jnp.bfloat16
MESH = pl.DeviceIdType.MESH


def group_rms(values, width):
    lane = lax.broadcasted_iota(jnp.int32, values.shape, 1)
    squares, scale = values * values, 0.0
    for start in range(0, values.shape[1], width):
        inside = (lane >= start) & (lane < start + width)
        mean = jnp.sum(jnp.where(inside, squares, 0.0), axis=-1, keepdims=True) * (1.0 / width)
        scale = jnp.where(inside, lax.rsqrt(mean + EPS), scale)
    return values * scale


def one_minus_exp(y):
    series = y * (1 + y / 2 * (1 + y / 3 * (1 + y / 4 * (1 + y / 5 * (1 + y / 6 * (1 + y / 7))))))
    return -jnp.where(y > -0.4, series, jnp.exp(y) - 1.0)


def softplus(x):
    u = jnp.exp(-jnp.abs(x))
    s = u / (2.0 + u)
    q = s * s
    series = 1.0 / 17
    for odd in (15, 13, 11, 9, 7, 5, 3, 1):
        series = series * q + 1.0 / odd
    return jnp.maximum(x, 0.0) + 2.0 * s * series


def sigmoid(x):
    return 1.0 / (1.0 + jnp.exp(-x))


def gelu(x):
    return 0.5 * x * (1.0 + jnp.tanh(0.7978845608028654 * (x + 0.044715 * x * x * x)))


def dot(a, b):
    return jnp.dot(a, b, preferred_element_type=F32)


def kernel(
    dims,
    x_any, norm_ref, wq_any, wk_any, wv_any, qg_ref, kg_ref, fc_ref, wr_any, wg_any, cw_ref,
    dgw_ref, igw_ref, dp_ref, de_any, ag_ref, rg_ref, oa_any, or_any,
    out_ref,
    x_ref, wq_ref, wr_ref, wg_ref, de_ref, wall, loads, xall, xsend, kvsrc, kvw, rw, qw, gw, kv_all, scanned, deg, rin, halo, st_all, act, gath, acc,
    zs, zr, fs, fr, xas, xar, xbs, xbr, xcs, xcr, xds, xdr, des, der, kvs, kvr, kps, kpr, hs, hr, ss, sr,
    acs, acr, ps, pr, qs, qr, ws, wr,
):
    n, nt, span, head_dim, flip = dims
    no, nto, ng = n // 2, nt // 2, n // 4
    me = lax.axis_index("sp")
    outer, inner = lax.div(me, 2), lax.rem(me, 2)
    grp, mem = lax.div(outer, 2), lax.rem(outer, 2)
    opp, omem = 1 - inner, 1 - mem
    mate = outer * 2 + opp
    pair = (grp * 2 + omem) * 2 + inner
    cross = (grp * 2 + omem) * 2 + opp
    tme = lax.axis_index("tp")
    touter, tinner = lax.div(tme, 2), lax.rem(tme, 2)
    tmate = touter * 2 + (1 - tinner)
    kr, channels = wq_ref.shape
    kvc = wk_any.shape[0 if flip else 1]
    width = x_ref.shape[1]
    half = channels // 2
    quarter = width // nt
    heads = half // head_dim
    taps = cw_ref.shape[0]
    gp = 4 * span

    def rows_of(i, size):
        return pl.ds(pl.multiple_of(i * size, size), size)

    def partner(d):
        who, bit = 0, 1
        while bit < no:
            own = lax.rem(lax.div(outer, bit), 2)
            who = who + bit * (1 - own if d & bit else own)
            bit *= 2
        return who

    def copy(src, dst, send, recv, **where):
        return pltpu.make_async_remote_copy(
            src_ref=src, dst_ref=dst, send_sem=send, recv_sem=recv, device_id=where, device_id_type=MESH
        )

    out_cols = rows_of(tme, out_ref.shape[1])
    staged = [
        pltpu.make_async_copy(src, dst, loads.at[i])
        for i, (src, dst) in enumerate((
            (x_any, x_ref), (wk_any, kvsrc.at[0]), (wv_any, kvsrc.at[1]), (wr_any, wr_ref), (wq_any, wq_ref),
            (wg_any, wg_ref), (de_any, de_ref), (oa_any.at[:, out_cols], wall.at[0, tme]), (or_any.at[:, out_cols], wall.at[1, tme]),
        ))
    ]
    for load in staged:
        load.start()
    barrier = pltpu.get_barrier_semaphore()
    for d in range(1, n):
        pl.semaphore_signal(barrier, inc=1, device_id={"sp": lax.rem(me + d, n)}, device_id_type=MESH)
    for d in range(1, nt):
        pl.semaphore_signal(barrier, inc=1, device_id={"tp": lax.rem(tme + d, nt)}, device_id_type=MESH)

    mine_block, mate_block = mem * 2 + inner, mem * 2 + opp
    pair_block, cross_block = omem * 2 + inner, omem * 2 + opp
    my_half, my_rows = rows_of(mem, half), rows_of(me, kr)
    my_cols = rows_of(tme, quarter)

    staged[0].wait()

    def scale_rows(seq):
        x = x_ref[rows_of(seq, span), :].astype(F32)
        return lax.rsqrt(jnp.mean(x * x, axis=-1, keepdims=True) + EPS)

    xsend[...] = (
        x_ref[rows_of(opp, span), my_cols].astype(F32) * scale_rows(opp) * norm_ref[:, my_cols]
    ).astype(BF16)
    xall[mine_block] = (x_ref[rows_of(inner, span), :].astype(F32) * scale_rows(inner) * norm_ref[...]).astype(BF16)
    for load in staged[1:]:
        load.wait()
    pl.semaphore_wait(barrier, n - 1 + nt - 1)

    weights = (None, wr_ref, wq_ref, wg_ref)
    buffers = (kvw, rw, qw, gw)

    def place(c, who):
        return kvw.at[:, rows_of(who, kr)] if c == 0 and flip else buffers[c].at[rows_of(who, kr), :]

    def origin(c, member):
        return kvsrc.at[member] if c == 0 else weights[c].at[:, rows_of(member, half)]

    def outward(c, d):
        to = partner(d)
        return copy(origin(c, lax.rem(to, 2)), place(c, me), zs.at[c, d - 1], zr.at[c, d - 1], sp=to * 2 + inner)

    def inward(c, d):
        who = partner(d) * 2 + inner
        return copy(place(c, who), place(c, who), zs.at[c, d - 1], zr.at[c, d - 1], sp=mate)

    def across(c, d, who, src=None):
        return copy(place(c, who) if src is None else src, place(c, who), fs.at[c, d], fr.at[c, d], sp=mate)

    def send_z(c):
        for d in range(1, no):
            outward(c, d).start()

    def send_y(c):
        across(c, 0, me, origin(c, mem)).start()

    def forward(c, which=range(1, no)):
        for d in which:
            inward(c, d).wait_recv()
            across(c, d, partner(d) * 2 + inner).start()

    def finish(c):
        for d in range(no):
            across(c, d, partner(d) * 2 + opp).wait_recv()

    def drain(c):
        for d in range(1, no):
            outward(c, d).wait_send()
        across(c, 0, me, origin(c, mem)).wait_send()
        for d in range(1, no):
            across(c, d, partner(d) * 2 + inner).wait_send()

    def piece_of(block, who=None):
        return xall.at[block, :, my_cols if who is None else rows_of(who, quarter)]

    to_mate_x = copy(xsend, piece_of(mine_block), xas, xar, sp=mate)
    to_pair_x = [
        copy(piece_of(mine_block), piece_of(mine_block), xbs.at[0], xbr.at[0], sp=pair),
        copy(piece_of(mate_block), piece_of(mate_block), xbs.at[1], xbr.at[1], sp=pair),
    ]
    shared = (mate_block, pair_block, cross_block)

    def to_far_x(k, d):
        far = lax.rem(touter + d, nto) * 2 + tinner
        return copy(piece_of(shared[k]), piece_of(shared[k]), xcs.at[k, d - 1], xcr.at[k, d - 1], tp=far)

    def to_core_x(k, d):
        ref = piece_of(shared[k], lax.rem(touter + nto - d, nto) * 2 + tinner)
        return copy(ref, ref, xds.at[k, d], xdr.at[k, d], tp=tmate)

    def spread(k):
        for d in range(1, nto):
            to_far_x(k, d).start()
        to_core_x(k, 0).start()

    def extra(i):
        to, seq, member = ((mate, opp, mem), (pair, inner, omem), (cross, opp, omem))[i]
        src = de_ref.at[rows_of(seq, span), rows_of(member, half)]
        return copy(src, deg.at[mine_block], des.at[i], der.at[i], sp=to)

    def out_weights(a, d, arriving=False):
        to, who = lax.rem(tme + d, nt), lax.rem(tme + nt - d, nt) if arriving else tme
        src = wall.at[a, who] if arriving else (oa_any, or_any)[a].at[:, rows_of(to, out_ref.shape[1])]
        return copy(src, wall.at[a, who], ws.at[a, d - 1], wr.at[a, d - 1], tp=to)

    to_mate_x.start()
    to_pair_x[0].start()
    send_z(0)
    deg[mine_block] = de_ref[rows_of(inner, span), my_half]
    if flip:
        kvw[:, my_rows] = kvsrc[mem]
    else:
        kvw[my_rows, :] = kvsrc[mem]
    rw[my_rows, :] = wr_ref[:, my_half]
    qw[my_rows, :] = wq_ref[:, my_half]
    gw[my_rows, :] = wg_ref[:, my_half]

    to_mate_x.wait_recv()
    to_pair_x[1].start()
    spread(0)
    send_y(0)
    send_y(1)
    to_pair_x[0].wait_recv()
    spread(1)
    forward(0, (1,))
    send_y(2)
    send_y(3)
    to_pair_x[1].wait_recv()
    spread(2)
    for a in range(2):
        for d in range(1, nt):
            out_weights(a, d).start()
    send_z(1)
    send_z(2)
    forward(0, range(2, no))
    forward(1, (1,))
    for i in range(3):
        extra(i).start()
    forward(1, range(2, no - 1))
    for k in range(3):
        for d in range(1, nto):
            to_far_x(k, d).wait_recv()
            to_core_x(k, d).start()
    forward(1, (no - 1,))
    for k in range(3):
        for d in range(nto):
            to_core_x(k, d).wait_recv()
    finish(0)

    def normed():
        return xall[...].reshape(gp, width)

    kv = lax.dot_general(normed(), kvw[...], (((1,), (1 if flip else 0,)), ((), ())), preferred_element_type=F32)
    kv = jnp.where(mem == 0, group_rms(kv, head_dim) * kg_ref[...], kv).astype(BF16)
    kv_all[mem, grp] = jnp.concatenate([kv[: gp // 2], kv[gp // 2 :]], axis=1)

    def kv_copy(d, who):
        to, ref = lax.rem(grp + d, ng) * 4 + mem * 2 + inner, kv_all.at[mem, who]
        return copy(ref, ref, kvs.at[d - 1], kvr.at[d - 1], sp=to)

    def kv_pair(d, member, who):
        ref = kv_all.at[member, who]
        return copy(ref, ref, kps.at[d], kpr.at[d], sp=pair)

    def state_copy(d, who):
        to = lax.rem(grp + d, ng) * 4 + mem * 2 + inner
        return copy(st_all.at[who], st_all.at[who], ss.at[d - 1], sr.at[d - 1], sp=to)

    def later(make, act_on):
        for d in range(1, ng):
            @pl.when(grp + d < ng)
            def _(d=d):
                act_on(make(d, grp))

    def earlier(make):
        for d in range(1, ng):
            @pl.when(grp >= d)
            def _(d=d):
                make(d, lax.rem(grp + ng - d, ng)).wait_recv()

    kv_pair(0, mem, grp).start()
    later(kv_copy, lambda c: c.start())
    send_z(3)
    forward(2, range(1, no - 1))

    finish(1)
    rec = dot(normed(), rw[...]).astype(BF16).astype(F32)
    rin[pl.ds(8, gp), :] = rec
    halo[0] = rec[gp - 8 : gp]
    halo[1] = jnp.zeros_like(halo[1])
    halo_copy = copy(halo.at[0], halo.at[2], hs, hr, sp=lax.rem(grp + 1, ng) * 4 + mem * 2 + inner)

    @pl.when(grp + 1 < ng)
    def _():
        halo_copy.start()

    lb = dgw_ref.shape[1]

    def recur():
        for i, block in ((0, mate_block), (1, pair_block), (2, cross_block)):
            copy(deg.at[block], deg.at[block], des.at[i], der.at[i], sp=mate).wait_recv()
        rin[pl.ds(0, 8), :] = halo[1]
        cw = cw_ref[:, my_half].astype(F32)
        conv = jnp.zeros((gp, half), F32)
        for tap in range(taps):
            conv = conv + rin[pl.ds(8 - (taps - 1) + tap, gp), :] * cw[tap : tap + 1]
        conv = conv.astype(BF16)
        nb = half // lb
        gate_decay = jnp.concatenate([dot(conv[:, i * lb : (i + 1) * lb], dgw_ref[mem * nb + i]) for i in range(nb)], axis=1)
        gate_input = jnp.concatenate([dot(conv[:, i * lb : (i + 1) * lb], igw_ref[mem * nb + i]) for i in range(nb)], axis=1)
        log_decay = -LRU_CONST * sigmoid(gate_decay) * softplus(-dp_ref[:, my_half]) + deg[...].reshape(gp, half)
        state = jnp.sqrt(one_minus_exp(2.0 * log_decay)) * sigmoid(gate_input) * conv.astype(F32)
        decay = jnp.exp(log_decay)
        time = lax.broadcasted_iota(jnp.int32, state.shape, 0)
        shift = 1
        while shift < gp:
            if shift < 8:
                seen = time >= shift
                state = state + decay * jnp.where(seen, pltpu.roll(state, shift, 0), 0.0)
                decay = decay * jnp.where(seen, pltpu.roll(decay, shift, 0), 1.0)
            else:
                moved = state[shift:] + decay[shift:] * state[: gp - shift]
                faded = decay[shift:] * decay[: gp - shift]
                state = jnp.concatenate([state[:shift], moved], axis=0)
                decay = jnp.concatenate([decay[:shift], faded], axis=0)
            shift *= 2
        scanned[0] = decay
        scanned[1] = state
        st_all[grp, pl.ds(0, 1), :] = decay[gp - 1 : gp]
        st_all[grp, pl.ds(1, 1), :] = state[gp - 1 : gp]
        later(state_copy, lambda c: c.start())

    forward(2, (no - 1,))
    @pl.when(grp == 0)
    def _():
        recur()

    for d in range(1, ng):
        @pl.when(grp >= d)
        def _(d=d):
            who = lax.rem(grp + ng - d, ng)
            kv_copy(d, who).wait_recv()
            kv_pair(d, mem, who).start()

    forward(3, range(1, 2))
    finish(2)
    scaling = head_dim ** (-0.5)
    query = dot(normed(), qw[...])
    gains = jnp.concatenate([qg_ref[...]] * heads, axis=1)
    query = ((group_rms(query, head_dim) * gains).astype(BF16) * scaling).astype(BF16)

    forward(3, range(2, no))
    kv_pair(0, omem, grp).wait_recv()
    def attend(carried, q, kb, vb, fade_row, mask):
        top, total, accum = carried
        s = lax.dot_general(q, kb, (((1,), (1,)), ((), ())), preferred_element_type=F32) - fade_row
        if mask is not None:
            s = jnp.where(mask, s, -jnp.inf)
        new_top = jnp.maximum(top, jnp.max(s, axis=-1, keepdims=True))
        w = jnp.exp(s - new_top)
        fade = jnp.exp(top - new_top)
        total = total * fade + jnp.sum(w, axis=-1, keepdims=True)
        return new_top, total, accum * fade + dot(w.astype(BF16), vb)

    qb = gp // 2
    jobs = [(h, i) for h in range(heads) for i in range(2)]

    def heads_of(which, j):
        packed = kv_all[which, j]
        return jnp.concatenate([packed[:, :kvc], packed[:, kvc:]], axis=0)

    def keys_of(j):
        k = heads_of(0, j)
        zero = jnp.zeros_like(k)
        return [jnp.concatenate([k if x == h else zero for x in range(heads)], axis=1) for h in range(heads)]

    k_own, v_own = keys_of(grp), heads_of(1, grp)
    carried = []
    for h, i in jobs:
        size = (i + 1) * qb
        kb, vb = k_own[h][:size], v_own[:size]
        fade_row = fc_ref[inner, pl.ds(mem * heads + h, 1), pl.ds(pl.multiple_of(grp * gp, gp), size)]
        mask = i * qb + lax.broadcasted_iota(jnp.int32, (qb, size), 0) >= lax.broadcasted_iota(jnp.int32, (qb, size), 1)
        start = (jnp.full((qb, 1), -1e30, F32), jnp.zeros((qb, 1), F32), jnp.zeros((qb, head_dim), F32))
        carried.append(attend(start, query[i * qb : size], kb, vb, fade_row, mask))

    for d in range(1, ng):
        @pl.when(grp >= d)
        def _(d=d):
            kv_pair(d, omem, lax.rem(grp + ng - d, ng)).wait_recv()

    def step(j, carried):
        result = []
        keys, vb = keys_of(j), heads_of(1, j)
        for (h, i), state_of in zip(jobs, carried):
            fade_row = fc_ref[inner, pl.ds(mem * heads + h, 1), pl.ds(pl.multiple_of(j * gp, gp), gp)]
            result.append(attend(state_of, query[i * qb : (i + 1) * qb], keys[h], vb, fade_row, None))
        return tuple(result)

    carried = lax.fori_loop(0, grp, step, tuple(carried))
    columns = []
    for h in range(heads):
        columns.append(jnp.concatenate([c[2] * (1.0 / c[1]) for (hh, i), c in zip(jobs, carried) if hh == h], axis=0))
    attended = group_rms(jnp.concatenate(columns, axis=1), head_dim) * ag_ref[:, my_half]

    def act_copy(a, i):
        to, block = ((mate, mate_block), (pair, pair_block), (cross, cross_block))[i]
        return copy(
            act.at[a, block], gath.at[a, tme, rows_of(inner, span), my_half], acs.at[a, i], acr.at[a, i], sp=to
        )

    def act_from(a, i):
        seq, member = ((opp, mem), (inner, omem), (opp, omem))[i]
        ref = gath.at[a, tme, rows_of(seq, span), rows_of(member, half)]
        return copy(ref, ref, acs.at[a, i], acr.at[a, i], sp=mate)

    def hand_out(a, values):
        act[a] = values.astype(BF16).reshape(4, span, half)
        for i in range(3):
            act_copy(a, i).start()
        gath[a, tme, rows_of(inner, span), my_half] = act[a, mine_block]

    hand_out(0, attended)

    @pl.when(grp > 0)
    def _():
        halo_copy.wait_recv()
        halo[1] = halo[2]
        recur()

    earlier(state_copy)

    def enter(j, e):
        return st_all[j, pl.ds(0, 1), :] * e + st_all[j, pl.ds(1, 1), :]

    entering = lax.fori_loop(0, grp, enter, jnp.zeros((1, half), F32))
    whole_state = scanned[1] + scanned[0] * entering
    finish(3)
    gated = whole_state * gelu(dot(normed(), gw[...]))

    def far_of(d):
        return lax.rem(touter + nto + d, nto) * 2

    def to_far(a, d):
        return copy(gath.at[a, tme], gath.at[a, tme], qs.at[a, d - 1], qr.at[a, d - 1], tp=far_of(d) + tinner)

    def to_core(a, d):
        ref = gath.at[a, far_of(-d) + tinner]
        return copy(ref, ref, ps.at[a, d], pr.at[a, d], tp=tmate)

    def gather(a):
        for i in range(3):
            act_from(a, i).wait_recv()
        for d in range(1, nto):
            to_far(a, d).start()
        to_core(a, 0).start()

    def relay(a):
        for d in range(1, nto):
            ref = gath.at[a, far_of(-d) + tinner]
            copy(ref, ref, qs.at[a, d - 1], qr.at[a, d - 1], tp=tmate).wait_recv()
            to_core(a, d).start()

    def arrive(a, d):
        ref = gath.at[a, far_of(-d) + 1 - tinner]
        copy(ref, ref, ps.at[a, d], pr.at[a, d], tp=tmate).wait_recv()

    def term(a, who):
        return dot(gath[a, who], wall[a, who])

    gather(0)
    hand_out(1, group_rms(gated, lb) * rg_ref[:, my_half])
    gather(1)
    relay(0)
    for a in range(2):
        for d in range(1, nt):
            out_weights(a, d, True).wait_recv()
    acc[...] = term(0, tme)
    for d in range(nto):
        arrive(0, d)
        acc[...] += term(0, far_of(-d) + 1 - tinner)
        if d:
            acc[...] += term(0, far_of(-d) + tinner)
    acc[...] += term(1, tme)
    relay(1)
    for d in range(1, nto):
        acc[...] += term(1, far_of(-d) + tinner)
    arrive(1, 0)
    acc[...] += term(1, tmate)
    for d in range(1, nto):
        arrive(1, d)
        acc[...] += term(1, far_of(-d) + 1 - tinner)
    out_ref[...] = acc[...].astype(BF16)
    for c in range(4):
        drain(c)
    to_mate_x.wait_send()
    for c in to_pair_x:
        c.wait_send()
    for k in range(3):
        extra(k).wait_send()
        for d in range(1, nto):
            to_far_x(k, d).wait_send()
        for d in range(nto):
            to_core_x(k, d).wait_send()
    later(kv_copy, lambda c: c.wait_send())
    kv_pair(0, mem, grp).wait_send()
    for d in range(1, ng):
        @pl.when(grp >= d)
        def _(d=d):
            kv_pair(d, mem, lax.rem(grp + ng - d, ng)).wait_send()

    later(state_copy, lambda c: c.wait_send())

    @pl.when(grp + 1 < ng)
    def _():
        halo_copy.wait_send()

    for a in range(2):
        for i in range(3):
            act_copy(a, i).wait_send()
    for a in range(2):
        for d in range(1, nt):
            out_weights(a, d).wait_send()
        for d in range(1, nto):
            to_far(a, d).wait_send()
        for d in range(nto):
            to_core(a, d).wait_send()


def body(
    n, nt,
    inputs, norm_gain, query_weight, key_weight, value_weight, query_gain, key_gain, forget_cache,
    rec_in_weight, rec_gate_weight, conv_weight, decay_gate_weight, input_gate_weight, decay_param,
    decay_extra, attn_out_gain, rec_out_gain, out_att_weight, out_rec_weight,
):
    seqs, span, width = inputs.shape
    assert seqs == 2 and n % 4 == 0 and nt % 2 == 0 and key_weight.shape[1] == query_gain.shape[0]
    rows = seqs * span
    head_dim = query_gain.shape[0]
    channels = rec_in_weight.shape[1]
    qc, kvc = query_weight.shape[1], key_weight.shape[1]
    half = channels // 2
    cols = out_att_weight.shape[1] // nt
    flip = query_weight.shape[0] % 128 == 0
    kv_weights = [w.T if flip else w for w in (key_weight, value_weight)]
    no, nto, ng = n // 2, nt // 2, n // 4
    dma = pltpu.SemaphoreType.DMA
    vmem, far = pl.BlockSpec(memory_space=pltpu.VMEM), pl.BlockSpec(memory_space=pl.ANY)
    out = pl.pallas_call(
        functools.partial(kernel, (n, nt, span, head_dim, flip)),
        out_shape=jax.ShapeDtypeStruct((rows, cols), BF16),
        in_specs=[far if i in (0, 2, 3, 4, 8, 9, 14, 17, 18) else vmem for i in range(19)],
        out_specs=vmem,
        scratch_shapes=[
            pltpu.VMEM((rows, width), BF16),
            pltpu.VMEM(query_weight.shape, BF16),
            pltpu.VMEM(rec_in_weight.shape, BF16),
            pltpu.VMEM(rec_gate_weight.shape, BF16),
            pltpu.VMEM((rows, channels), F32),
            pltpu.VMEM((2, nt, channels, cols), BF16),
            dma((9,)),
            pltpu.VMEM((4, span, width), BF16),
            pltpu.VMEM((span, width // nt), BF16),
            pltpu.VMEM((2, *kv_weights[0].shape), BF16),
            pltpu.VMEM((kvc, width) if flip else (width, kvc), BF16),
            pltpu.VMEM((width, half), BF16),
            pltpu.VMEM((width, half), BF16),
            pltpu.VMEM((width, half), BF16),
            pltpu.VMEM((2, ng, 2 * span, 2 * kvc), BF16),
            pltpu.VMEM((2, 4 * span, half), F32),
            pltpu.VMEM((4, span, half), F32),
            pltpu.VMEM((4 * span + 8, half), F32),
            pltpu.VMEM((3, 8, half), F32),
            pltpu.VMEM((ng, 8, half), F32),
            pltpu.VMEM((2, 4, span, half), BF16),
            pltpu.VMEM((2, nt, rows, channels), BF16),
            pltpu.VMEM((rows, cols), F32),
            dma((4, no)), dma((4, no)), dma((4, no)), dma((4, no)),
            dma, dma, dma((2,)), dma((2,)), dma((3, nto)), dma((3, nto)), dma((3, nto)), dma((3, nto)),
            dma((3,)), dma((3,)), dma((ng,)), dma((ng,)), dma((ng,)), dma((ng,)), dma, dma, dma((ng,)), dma((ng,)),
            dma((2, 3)), dma((2, 3)), dma((2, nto)), dma((2, nto)), dma((2, nto)), dma((2, nto)),
            dma((2, nt)), dma((2, nt)),
        ],
        compiler_params=pltpu.CompilerParams(
            collective_id=0, has_side_effects=True, vmem_limit_bytes=60 * 1024 * 1024
        ),
    )(
        inputs.reshape(rows, width), norm_gain.reshape(1, width), query_weight, *kv_weights,
        query_gain.reshape(1, head_dim), key_gain.reshape(1, head_dim), forget_cache,
        rec_in_weight, rec_gate_weight, conv_weight, decay_gate_weight, input_gate_weight,
        decay_param.reshape(1, channels), decay_extra.reshape(rows, channels),
        attn_out_gain.reshape(1, qc), rec_out_gain.reshape(1, channels), out_att_weight, out_rec_weight,
    )
    return out.reshape(seqs, span, cols)


def solution(mesh):
    return jax.shard_map(
        functools.partial(body, mesh.shape["sp"], mesh.shape["tp"]),
        mesh=mesh,
        in_specs=(
            P(None, "sp", None), P(), P("sp", "tp"), P("sp", "tp"), P("sp", "tp"), P(), P(),
            P(None, "tp", None), P("sp", "tp"), P("sp", "tp"), P(None, "tp"), P("tp", None, None),
            P("tp", None, None), P("tp"), P(None, "sp", "tp"), P("tp"), P("tp"), P("tp", None), P("tp", None),
        ),
        out_specs=P(None, "sp", "tp"),
        check_vma=False,
    )
```

```python
import functools

import jax
import jax.numpy as jnp
from jax import lax
from jax.experimental import pallas as pl
from jax.experimental.pallas import tpu as pltpu
from jax.sharding import PartitionSpec as P

LRU_CONST = 8.0
EPS = 1e-06
F32 = jnp.float32
BF16 = jnp.bfloat16
MESH = pl.DeviceIdType.MESH


def group_rms(values, width):
    lane = lax.broadcasted_iota(jnp.int32, values.shape, 1)
    squares, scale = values * values, 0.0
    for start in range(0, values.shape[1], width):
        inside = (lane >= start) & (lane < start + width)
        mean = jnp.sum(jnp.where(inside, squares, 0.0), axis=-1, keepdims=True) * (1.0 / width)
        scale = jnp.where(inside, lax.rsqrt(mean + EPS), scale)
    return values * scale


def one_minus_exp(y):
    series = y * (1 + y / 2 * (1 + y / 3 * (1 + y / 4 * (1 + y / 5 * (1 + y / 6 * (1 + y / 7))))))
    return -jnp.where(y > -0.4, series, jnp.exp(y) - 1.0)


def softplus(x):
    u = jnp.exp(-jnp.abs(x))
    s = u / (2.0 + u)
    q = s * s
    series = 1.0 / 17
    for odd in (15, 13, 11, 9, 7, 5, 3, 1):
        series = series * q + 1.0 / odd
    return jnp.maximum(x, 0.0) + 2.0 * s * series


def sigmoid(x):
    return 1.0 / (1.0 + jnp.exp(-x))


def gelu(x):
    return 0.5 * x * (1.0 + jnp.tanh(0.7978845608028654 * (x + 0.044715 * x * x * x)))


def dot(a, b):
    return jnp.dot(a, b, preferred_element_type=F32)


def kernel(
    dims,
    x_any, norm_any, wq_any, wk_any, wv_any, qg_any, kg_any, fc_any, wr_any, wg_any, cw_any,
    dgw_any, igw_any, dp_any, de_any, ag_any, rg_any, oa_any, or_any,
    out_ref,
    x_ref, wq_ref, wr_ref, wg_ref, de_ref, wall, norm_ref, qg_ref, kg_ref, fc_ref, cw_ref, dgw_ref, igw_ref, dp_ref,
    ag_ref, rg_ref, loads, xall, xsend, kvsrc, kvw, rw, qw, gw, kv_all, scanned, deg, rin, halo, st_all, act, gath, acc,
    zs, zr, fr, xs, xar, xbr, xcr, xdr, des, der, kvs, kvr, kps, kpr, hs, hr, ss, sr,
    acs, acr, ps, pr, qr, ws, wr,
):
    n, nt, span, head_dim, flip = dims
    no, nto, ng = n // 2, nt // 2, n // 4
    me = lax.axis_index("sp")
    outer, inner = lax.div(me, 2), lax.rem(me, 2)
    grp, mem = lax.div(outer, 2), lax.rem(outer, 2)
    opp, omem = 1 - inner, 1 - mem
    mate = outer * 2 + opp
    pair = (grp * 2 + omem) * 2 + inner
    cross = (grp * 2 + omem) * 2 + opp
    tme = lax.axis_index("tp")
    touter, tinner = lax.div(tme, 2), lax.rem(tme, 2)
    tmate = touter * 2 + (1 - tinner)
    kr, channels = wq_ref.shape
    kvc = wk_any.shape[0 if flip else 1]
    width = x_ref.shape[1]
    half = channels // 2
    quarter = width // nt
    heads = half // head_dim
    taps = cw_ref.shape[0]
    gp = 4 * span

    def rows_of(i, size):
        return pl.ds(pl.multiple_of(i * size, size), size)

    def partner(d):
        who, bit = 0, 1
        while bit < no:
            own = lax.rem(lax.div(outer, bit), 2)
            who = who + bit * (1 - own if d & bit else own)
            bit *= 2
        return who

    def copy(src, dst, send, recv, **where):
        return pltpu.make_async_remote_copy(
            src_ref=src, dst_ref=dst, send_sem=send, recv_sem=recv, device_id=where, device_id_type=MESH
        )

    out_cols = rows_of(tme, out_ref.shape[1])
    staged = [
        pltpu.make_async_copy(src, dst, loads.at[i])
        for i, (src, dst) in enumerate((
            (x_any, x_ref), (norm_any, norm_ref), (wk_any, kvsrc.at[0]), (wv_any, kvsrc.at[1]), (wr_any, wr_ref), (wq_any, wq_ref),
            (wg_any, wg_ref), (de_any, de_ref), (oa_any.at[:, out_cols], wall.at[0, tme]), (or_any.at[:, out_cols], wall.at[1, tme]),
            (qg_any, qg_ref), (kg_any, kg_ref), (fc_any, fc_ref), (cw_any, cw_ref), (dgw_any, dgw_ref),
            (igw_any, igw_ref), (dp_any, dp_ref), (ag_any, ag_ref), (rg_any, rg_ref),
        ))
    ]
    for load in staged:
        load.start()
    barrier = pltpu.get_barrier_semaphore()
    for d in range(1, n):
        pl.semaphore_signal(barrier, inc=1, device_id={"sp": lax.rem(me + d, n)}, device_id_type=MESH)
    for d in range(1, nt):
        pl.semaphore_signal(barrier, inc=1, device_id={"tp": lax.rem(tme + d, nt)}, device_id_type=MESH)

    mine_block, mate_block = mem * 2 + inner, mem * 2 + opp
    pair_block, cross_block = omem * 2 + inner, omem * 2 + opp
    my_half, my_rows = rows_of(mem, half), rows_of(me, kr)
    my_cols = rows_of(tme, quarter)

    staged[0].wait()
    staged[1].wait()

    def scale_rows(seq):
        x = x_ref[rows_of(seq, span), :].astype(F32)
        return lax.rsqrt(jnp.mean(x * x, axis=-1, keepdims=True) + EPS)

    xsend[...] = (
        x_ref[rows_of(opp, span), my_cols].astype(F32) * scale_rows(opp) * norm_ref[:, my_cols]
    ).astype(BF16)
    xall[mine_block] = (x_ref[rows_of(inner, span), :].astype(F32) * scale_rows(inner) * norm_ref[...]).astype(BF16)
    for load in staged[2:]:
        load.wait()
    pl.semaphore_wait(barrier, n - 1 + nt - 1)

    weights = (None, wr_ref, wq_ref, wg_ref)
    buffers = (kvw, rw, qw, gw)

    def place(c, who):
        return kvw.at[:, rows_of(who, kr)] if c == 0 and flip else buffers[c].at[rows_of(who, kr), :]

    def origin(c, member):
        return kvsrc.at[member] if c == 0 else weights[c].at[:, rows_of(member, half)]

    def outward(c, d):
        to = partner(d)
        return copy(origin(c, lax.rem(to, 2)), place(c, me), zs.at[c], zr.at[c, d - 1], sp=to * 2 + inner)

    def inward(c, d):
        who = partner(d) * 2 + inner
        return copy(place(c, who), place(c, who), zs.at[c], zr.at[c, d - 1], sp=mate)

    def across(c, d, who, src=None):
        return copy(place(c, who) if src is None else src, place(c, who), zs.at[c], fr.at[c], sp=mate)

    line = no == 4
    middle = (outer == 1) | (outer == 2)

    def send_z(c, which=range(1, no)):
        for d in which:
            if line and c > 0 and d == no - 1:
                pl.when(jnp.logical_not(middle))(outward(c, d).start)
            else:
                outward(c, d).start()

    def send_y(c):
        across(c, 0, me, origin(c, mem)).start()

    def forward(c, which=range(1, no)):
        for d in which:
            inward(c, d).wait_recv()
            across(c, d, partner(d) * 2 + inner).start()

    def span_of(c, parts):
        return kvw.at[:, pl.ds(0, parts * kr)] if c == 0 and flip else buffers[c].at[pl.ds(0, parts * kr), :]

    def finish(c):
        copy(span_of(c, no), span_of(c, no), zs.at[c], fr.at[c], sp=mate).wait_recv()

    def drain(c):
        copy(span_of(c, n - 1), span_of(c, n - 1), zs.at[c], fr.at[c], sp=mate).wait_send()

    def piece_of(block, who=None):
        return xall.at[block, :, my_cols if who is None else rows_of(who, quarter)]

    to_mate_x = copy(xsend, piece_of(mine_block), xs, xar, sp=mate)
    to_pair_x = [
        copy(piece_of(mine_block), piece_of(mine_block), xs, xbr.at[0], sp=pair),
        copy(piece_of(mate_block), piece_of(mate_block), xs, xbr.at[1], sp=pair),
    ]
    shared = (mate_block, pair_block, cross_block)

    def to_far_x(k, d):
        far = lax.rem(touter + d, nto) * 2 + tinner
        return copy(piece_of(shared[k]), piece_of(shared[k]), xs, xcr.at[k, d - 1], tp=far)

    def to_core_x(k, d):
        ref = piece_of(shared[k], lax.rem(touter + nto - d, nto) * 2 + tinner)
        return copy(ref, ref, xs, xdr, tp=tmate)

    def spread(k):
        for d in range(1, nto):
            to_far_x(k, d).start()
        to_core_x(k, 0).start()

    def extra(i):
        to, seq, member = ((mate, opp, mem), (pair, inner, omem), (cross, opp, omem))[i]
        src = de_ref.at[rows_of(seq, span), rows_of(member, half)]
        return copy(src, deg.at[mine_block], des, der, sp=to)

    def out_weights(a, d):
        to = lax.rem(tme + d, nt)
        src = (oa_any, or_any)[a].at[:, rows_of(to, out_ref.shape[1])]
        return copy(src, wall.at[a, tme], ws, wr, tp=to)

    to_mate_x.start()
    to_pair_x[0].start()
    send_z(0)
    if line:
        for c in range(1, 4):
            pl.when(middle)(outward(c, no - 1).start)
    deg[mine_block] = de_ref[rows_of(inner, span), my_half]
    if flip:
        kvw[:, my_rows] = kvsrc[mem]
    else:
        kvw[my_rows, :] = kvsrc[mem]
    rw[my_rows, :] = wr_ref[:, my_half]
    qw[my_rows, :] = wq_ref[:, my_half]
    gw[my_rows, :] = wg_ref[:, my_half]

    to_mate_x.wait_recv()
    to_pair_x[1].start()
    spread(0)
    send_y(0)
    send_y(1)
    to_pair_x[0].wait_recv()
    spread(1)
    forward(0, (1,))
    send_y(2)
    send_y(3)
    to_pair_x[1].wait_recv()
    spread(2)
    for a in range(2):
        for d in range(1, nt):
            out_weights(a, d).start()
    send_z(1)
    send_z(2)
    forward(0, range(2, no))
    forward(1, (1,))
    for i in range(3):
        extra(i).start()
    forward(1, range(2, no - 1))
    for k in range(3):
        for d in range(1, nto):
            to_far_x(k, d).wait_recv()
            to_core_x(k, d).start()
    forward(1, (no - 1,))
    shares = xall.at[pl.ds(0, 3), :, pl.ds(0, nto * quarter)]
    copy(shares, shares, xs, xdr, tp=tmate).wait_recv()
    finish(0)

    def normed():
        return xall[...].reshape(gp, width)

    kv = lax.dot_general(normed(), kvw[...], (((1,), (1 if flip else 0,)), ((), ())), preferred_element_type=F32)
    kv = jnp.where(mem == 0, group_rms(kv, head_dim) * kg_ref[...], kv).astype(BF16)
    kv_all[mem, grp] = jnp.concatenate([kv[: gp // 2], kv[gp // 2 :]], axis=1)

    def kv_copy(d, who):
        to, ref = lax.rem(grp + d, ng) * 4 + mem * 2 + inner, kv_all.at[mem, who]
        return copy(ref, ref, kvs.at[d - 1], kvr.at[d - 1], sp=to)

    def kv_pair(d, member, who):
        ref = kv_all.at[member, who]
        return copy(ref, ref, kps.at[d], kpr.at[d], sp=pair)

    def state_copy(d, who):
        to = lax.rem(grp + d, ng) * 4 + mem * 2 + inner
        return copy(st_all.at[who], st_all.at[who], ss.at[d - 1], sr.at[d - 1], sp=to)

    def later(make, act_on):
        for d in range(1, ng):
            @pl.when(grp + d < ng)
            def _(d=d):
                act_on(make(d, grp))

    def earlier(make):
        for d in range(1, ng):
            @pl.when(grp >= d)
            def _(d=d):
                make(d, lax.rem(grp + ng - d, ng)).wait_recv()

    kv_pair(0, mem, grp).start()
    later(kv_copy, lambda c: c.start())
    send_z(3, (1,))
    forward(2, range(1, no - 1))

    finish(1)
    rec = dot(normed(), rw[...]).astype(BF16).astype(F32)
    rin[pl.ds(8, gp), :] = rec
    halo[0] = rec[gp - 8 : gp]
    halo[1] = jnp.zeros_like(halo[1])
    halo_copy = copy(halo.at[0], halo.at[2], hs, hr, sp=lax.rem(grp + 1, ng) * 4 + mem * 2 + inner)

    @pl.when(grp + 1 < ng)
    def _():
        halo_copy.start()

    send_z(3, range(2, no))
    lb = dgw_ref.shape[1]

    def recur():
        copy(deg.at[pl.ds(0, 3)], deg.at[pl.ds(0, 3)], des, der, sp=mate).wait_recv()
        rin[pl.ds(0, 8), :] = halo[1]
        cw = cw_ref[:, my_half].astype(F32)
        conv = jnp.zeros((gp, half), F32)
        for tap in range(taps):
            conv = conv + rin[pl.ds(8 - (taps - 1) + tap, gp), :] * cw[tap : tap + 1]
        conv = conv.astype(BF16)
        nb = half // lb
        gate_decay = jnp.concatenate([dot(conv[:, i * lb : (i + 1) * lb], dgw_ref[mem * nb + i]) for i in range(nb)], axis=1)
        gate_input = jnp.concatenate([dot(conv[:, i * lb : (i + 1) * lb], igw_ref[mem * nb + i]) for i in range(nb)], axis=1)
        log_decay = -LRU_CONST * sigmoid(gate_decay) * softplus(-dp_ref[:, my_half]) + deg[...].reshape(gp, half)
        state = jnp.sqrt(one_minus_exp(2.0 * log_decay)) * sigmoid(gate_input) * conv.astype(F32)
        decay = jnp.exp(log_decay)
        time = lax.broadcasted_iota(jnp.int32, state.shape, 0)
        shift = 1
        while shift < gp:
            if shift < 8:
                seen = time >= shift
                state = state + decay * jnp.where(seen, pltpu.roll(state, shift, 0), 0.0)
                decay = decay * jnp.where(seen, pltpu.roll(decay, shift, 0), 1.0)
            else:
                moved = state[shift:] + decay[shift:] * state[: gp - shift]
                faded = decay[shift:] * decay[: gp - shift]
                state = jnp.concatenate([state[:shift], moved], axis=0)
                decay = jnp.concatenate([decay[:shift], faded], axis=0)
            shift *= 2
        scanned[0] = decay
        scanned[1] = state
        st_all[grp, pl.ds(0, 1), :] = decay[gp - 1 : gp]
        st_all[grp, pl.ds(1, 1), :] = state[gp - 1 : gp]
        later(state_copy, lambda c: c.start())

    forward(2, (no - 1,))
    for d in range(1, ng):
        @pl.when(grp >= d)
        def _(d=d):
            who = lax.rem(grp + ng - d, ng)
            kv_copy(d, who).wait_recv()
            kv_pair(d, mem, who).start()

    @pl.when(grp > 0)
    def _():
        halo_copy.wait_recv()
        halo[1] = halo[2]

    recur()
    finish(2)
    scaling = head_dim ** (-0.5)
    query = dot(normed(), qw[...])
    gains = jnp.concatenate([qg_ref[...]] * heads, axis=1)
    query = ((group_rms(query, head_dim) * gains).astype(BF16) * scaling).astype(BF16)

    forward(3, (1,))
    kv_pair(0, omem, grp).wait_recv()
    def attend(carried, q, kb, vb, fade_row, mask):
        top, total, accum = carried
        s = lax.dot_general(q, kb, (((1,), (1,)), ((), ())), preferred_element_type=F32) - fade_row
        if mask is not None:
            s = jnp.where(mask, s, -jnp.inf)
        new_top = jnp.maximum(top, jnp.max(s, axis=-1, keepdims=True))
        w = jnp.exp(s - new_top)
        fade = jnp.exp(top - new_top)
        total = total * fade + jnp.sum(w, axis=-1, keepdims=True)
        return new_top, total, accum * fade + dot(w.astype(BF16), vb)

    qb = gp // 2
    jobs = [(h, i) for h in range(heads) for i in range(2)]

    def heads_of(which, j):
        packed = kv_all[which, j]
        return jnp.concatenate([packed[:, :kvc], packed[:, kvc:]], axis=0)

    def keys_of(j):
        k = heads_of(0, j)
        zero = jnp.zeros_like(k)
        return [jnp.concatenate([k if x == h else zero for x in range(heads)], axis=1) for h in range(heads)]

    k_own, v_own = keys_of(grp), heads_of(1, grp)
    carried = []
    for h, i in jobs:
        size = (i + 1) * qb
        kb, vb = k_own[h][:size], v_own[:size]
        fade_row = fc_ref[inner, pl.ds(mem * heads + h, 1), pl.ds(pl.multiple_of(grp * gp, gp), size)]
        mask = i * qb + lax.broadcasted_iota(jnp.int32, (qb, size), 0) >= lax.broadcasted_iota(jnp.int32, (qb, size), 1)
        start = (jnp.full((qb, 1), -1e30, F32), jnp.zeros((qb, 1), F32), jnp.zeros((qb, head_dim), F32))
        carried.append(attend(start, query[i * qb : size], kb, vb, fade_row, mask))

    forward(3, range(2, no))
    for d in range(1, ng):
        @pl.when(grp >= d)
        def _(d=d):
            kv_pair(d, omem, lax.rem(grp + ng - d, ng)).wait_recv()

    def step(j, carried):
        result = []
        keys, vb = keys_of(j), heads_of(1, j)
        for (h, i), state_of in zip(jobs, carried):
            fade_row = fc_ref[inner, pl.ds(mem * heads + h, 1), pl.ds(pl.multiple_of(j * gp, gp), gp)]
            result.append(attend(state_of, query[i * qb : (i + 1) * qb], keys[h], vb, fade_row, None))
        return tuple(result)

    carried = lax.fori_loop(0, grp, step, tuple(carried))
    columns = []
    for h in range(heads):
        columns.append(jnp.concatenate([c[2] * (1.0 / c[1]) for (hh, i), c in zip(jobs, carried) if hh == h], axis=0))
    attended = group_rms(jnp.concatenate(columns, axis=1), head_dim) * ag_ref[:, my_half]

    def act_copy(a, i):
        to, block = ((mate, mate_block), (pair, pair_block), (cross, cross_block))[i]
        return copy(
            act.at[a, block], gath.at[a, tme, rows_of(inner, span), my_half], acs, acr.at[a], sp=to
        )

    def act_from(a):
        copy(act.at[a, pl.ds(0, 3)], act.at[a, pl.ds(0, 3)], acs, acr.at[a], sp=mate).wait_recv()

    def hand_out(a, values):
        act[a] = values.astype(BF16).reshape(4, span, half)
        for i in range(3):
            act_copy(a, i).start()
        gath[a, tme, rows_of(inner, span), my_half] = act[a, mine_block]

    hand_out(0, attended)

    earlier(state_copy)

    def enter(j, e):
        return st_all[j, pl.ds(0, 1), :] * e + st_all[j, pl.ds(1, 1), :]

    entering = lax.fori_loop(0, grp, enter, jnp.zeros((1, half), F32))
    whole_state = scanned[1] + scanned[0] * entering
    finish(3)
    gated = whole_state * gelu(dot(normed(), gw[...]))

    def far_of(d):
        return lax.rem(touter + nto + d, nto) * 2

    def to_far(a, d):
        return copy(gath.at[a, tme], gath.at[a, tme], ps, qr.at[a, d - 1], tp=far_of(d) + tinner)

    def to_core(a, d):
        ref = gath.at[a, far_of(-d) + tinner]
        return copy(ref, ref, ps, pr.at[a, d], tp=tmate)

    def gather(a):
        act_from(a)
        for d in range(1, nto):
            to_far(a, d).start()
        to_core(a, 0).start()

    def relay(a):
        for d in range(1, nto):
            ref = gath.at[a, far_of(-d) + tinner]
            copy(ref, ref, ps, qr.at[a, d - 1], tp=tmate).wait_recv()
            to_core(a, d).start()

    def arrive(a, d):
        ref = gath.at[a, far_of(-d) + 1 - tinner]
        copy(ref, ref, ps, pr.at[a, d], tp=tmate).wait_recv()

    def term(a, who):
        return dot(gath[a, who], wall[a, who])

    hand_out(1, group_rms(gated, lb) * rg_ref[:, my_half])
    gather(0)
    gather(1)
    relay(0)
    copy(wall.at[:, pl.ds(0, nt - 1)], wall.at[:, pl.ds(0, nt - 1)], ws, wr, tp=tmate).wait_recv()
    acc[...] = term(0, tme)
    for d in range(nto):
        arrive(0, d)
        acc[...] += term(0, far_of(-d) + 1 - tinner)
        if d:
            acc[...] += term(0, far_of(-d) + tinner)
    acc[...] += term(1, tme)
    relay(1)
    for d in range(1, nto):
        acc[...] += term(1, far_of(-d) + tinner)
    arrive(1, 0)
    acc[...] += term(1, tmate)
    for d in range(1, nto):
        arrive(1, d)
        acc[...] += term(1, far_of(-d) + 1 - tinner)
    out_ref[...] = acc[...].astype(BF16)
    for c in range(4):
        drain(c)
    copy(xall.at[pl.ds(0, 3)], xall.at[pl.ds(0, 3)], xs, xar, sp=mate).wait_send()
    copy(deg.at[pl.ds(0, 3)], deg.at[pl.ds(0, 3)], des, der, sp=mate).wait_send()
    later(kv_copy, lambda c: c.wait_send())
    kv_pair(0, mem, grp).wait_send()
    for d in range(1, ng):
        @pl.when(grp >= d)
        def _(d=d):
            kv_pair(d, mem, lax.rem(grp + ng - d, ng)).wait_send()

    later(state_copy, lambda c: c.wait_send())

    @pl.when(grp + 1 < ng)
    def _():
        halo_copy.wait_send()

    copy(act.at[:, pl.ds(0, 3)], act.at[:, pl.ds(0, 3)], acs, acr.at[0], sp=mate).wait_send()
    copy(wall.at[:, pl.ds(0, nt - 1)], wall.at[:, pl.ds(0, nt - 1)], ws, wr, tp=tmate).wait_send()
    copy(gath.at[:, pl.ds(0, nt - 1)], gath.at[:, pl.ds(0, nt - 1)], ps, wr, tp=tmate).wait_send()


def body(
    n, nt,
    inputs, norm_gain, query_weight, key_weight, value_weight, query_gain, key_gain, forget_cache,
    rec_in_weight, rec_gate_weight, conv_weight, decay_gate_weight, input_gate_weight, decay_param,
    decay_extra, attn_out_gain, rec_out_gain, out_att_weight, out_rec_weight,
):
    seqs, span, width = inputs.shape
    assert seqs == 2 and n % 4 == 0 and nt % 2 == 0 and key_weight.shape[1] == query_gain.shape[0]
    rows = seqs * span
    head_dim = query_gain.shape[0]
    channels = rec_in_weight.shape[1]
    qc, kvc = query_weight.shape[1], key_weight.shape[1]
    half = channels // 2
    cols = out_att_weight.shape[1] // nt
    flip = query_weight.shape[0] % 128 == 0
    kv_weights = [w.T if flip else w for w in (key_weight, value_weight)]
    no, nto, ng = n // 2, nt // 2, n // 4
    dma = pltpu.SemaphoreType.DMA
    vmem, far = pl.BlockSpec(memory_space=pltpu.VMEM), pl.BlockSpec(memory_space=pltpu.HBM)
    out = pl.pallas_call(
        functools.partial(kernel, (n, nt, span, head_dim, flip)),
        out_shape=pltpu.VMEM((rows, cols), BF16),
        in_specs=[far] * 19,
        out_specs=vmem,
        scratch_shapes=[
            pltpu.VMEM((rows, width), BF16),
            pltpu.VMEM(query_weight.shape, BF16),
            pltpu.VMEM(rec_in_weight.shape, BF16),
            pltpu.VMEM(rec_gate_weight.shape, BF16),
            pltpu.VMEM((rows, channels), F32),
            pltpu.VMEM((2, nt, channels, cols), BF16),
            pltpu.VMEM((1, width), F32),
            pltpu.VMEM((1, head_dim), F32),
            pltpu.VMEM((1, head_dim), F32),
            pltpu.VMEM(forget_cache.shape, F32),
            pltpu.VMEM(conv_weight.shape, BF16),
            pltpu.VMEM(decay_gate_weight.shape, BF16),
            pltpu.VMEM(input_gate_weight.shape, BF16),
            pltpu.VMEM((1, channels), F32),
            pltpu.VMEM((1, qc), F32),
            pltpu.VMEM((1, channels), F32),
            dma((19,)),
            pltpu.VMEM((4, span, width), BF16),
            pltpu.VMEM((span, width // nt), BF16),
            pltpu.VMEM((2, *kv_weights[0].shape), BF16),
            pltpu.VMEM((kvc, width) if flip else (width, kvc), BF16),
            pltpu.VMEM((width, half), BF16),
            pltpu.VMEM((width, half), BF16),
            pltpu.VMEM((width, half), BF16),
            pltpu.VMEM((2, ng, 2 * span, 2 * kvc), BF16),
            pltpu.VMEM((2, 4 * span, half), F32),
            pltpu.VMEM((4, span, half), F32),
            pltpu.VMEM((4 * span + 8, half), F32),
            pltpu.VMEM((3, 8, half), F32),
            pltpu.VMEM((ng, 8, half), F32),
            pltpu.VMEM((2, 4, span, half), BF16),
            pltpu.VMEM((2, nt, rows, channels), BF16),
            pltpu.VMEM((rows, cols), F32),
            dma((4,)), dma((4, no - 1)), dma((4,)), dma, dma, dma((2,)), dma((3, nto - 1)), dma,
            dma, dma, dma((ng - 1,)), dma((ng - 1,)), dma((ng,)), dma((ng,)), dma, dma, dma((ng - 1,)), dma((ng - 1,)),
            dma, dma((2,)), dma, dma((2, nto)), dma((2, nto - 1)), dma, dma,
        ],
        compiler_params=pltpu.CompilerParams(
            collective_id=0, has_side_effects=True, vmem_limit_bytes=60 * 1024 * 1024
        ),
    )(
        inputs.reshape(rows, width), norm_gain.reshape(1, width), query_weight, *kv_weights,
        query_gain.reshape(1, head_dim), key_gain.reshape(1, head_dim), forget_cache,
        rec_in_weight, rec_gate_weight, conv_weight, decay_gate_weight, input_gate_weight,
        decay_param.reshape(1, channels), decay_extra.reshape(rows, channels),
        attn_out_gain.reshape(1, qc), rec_out_gain.reshape(1, channels), out_att_weight, out_rec_weight,
    )
    return out.reshape(seqs, span, cols)


def solution(mesh):
    return jax.shard_map(
        functools.partial(body, mesh.shape["sp"], mesh.shape["tp"]),
        mesh=mesh,
        in_specs=(
            P(None, "sp", None), P(), P("sp", "tp"), P("sp", "tp"), P("sp", "tp"), P(), P(),
            P(None, "tp", None), P("sp", "tp"), P("sp", "tp"), P(None, "tp"), P("tp", None, None),
            P("tp", None, None), P("tp"), P(None, "sp", "tp"), P("tp"), P("tp"), P("tp", None), P("tp", None),
        ),
        out_specs=P(None, "sp", "tp"),
        check_vma=False,
    )
```

```python
import functools

import jax
import jax.numpy as jnp
from jax import lax
from jax.experimental import pallas as pl
from jax.experimental.pallas import tpu as pltpu
from jax.sharding import PartitionSpec as P

LRU_CONST = 8.0
EPS = 1e-06
F32 = jnp.float32
BF16 = jnp.bfloat16
MESH = pl.DeviceIdType.MESH


def group_rms(values, width):
    lane = lax.broadcasted_iota(jnp.int32, values.shape, 1)
    squares, scale = values * values, 0.0
    for start in range(0, values.shape[1], width):
        inside = (lane >= start) & (lane < start + width)
        mean = jnp.sum(jnp.where(inside, squares, 0.0), axis=-1, keepdims=True) * (1.0 / width)
        scale = jnp.where(inside, lax.rsqrt(mean + EPS), scale)
    return values * scale


def one_minus_exp(y):
    series = y * (1 + y / 2 * (1 + y / 3 * (1 + y / 4 * (1 + y / 5 * (1 + y / 6 * (1 + y / 7))))))
    return -jnp.where(y > -0.4, series, jnp.exp(y) - 1.0)


def softplus(x):
    u = jnp.exp(-jnp.abs(x))
    s = u / (2.0 + u)
    q = s * s
    series = 1.0 / 17
    for odd in (15, 13, 11, 9, 7, 5, 3, 1):
        series = series * q + 1.0 / odd
    return jnp.maximum(x, 0.0) + 2.0 * s * series


def sigmoid(x):
    return 1.0 / (1.0 + jnp.exp(-x))


def gelu(x):
    return 0.5 * x * (1.0 + jnp.tanh(0.7978845608028654 * (x + 0.044715 * x * x * x)))


def dot(a, b):
    return jnp.dot(a, b, preferred_element_type=F32)


def kernel(
    dims,
    x_any, norm_any, wq_any, wk_any, wv_any, qg_any, kg_any, fc_any, wr_any, wg_any, cw_any,
    dgw_any, igw_any, dp_any, de_any, ag_any, rg_any, oa_any, or_any,
    out_ref,
    x_ref, wq_ref, wr_ref, wg_ref, de_ref, wall, norm_ref, qg_ref, kg_ref, fc_ref, cw_ref, dgw_ref, igw_ref, dp_ref,
    ag_ref, rg_ref, loads, xall, xsend, kvsrc, kvw, rw, qw, gw, kv_all, scanned, deg, rin, halo, st_all, act, gath, acc,
    zs, zr, fr, xs, xar, xbr, xcr, xdr, des, der, kvs, kvr, kps, kpr, hs, hr, ss, sr,
    acs, acr, ps, pr, qr, ws, wr,
):
    n, nt, span, head_dim, flip = dims
    no, nto, ng = n // 2, nt // 2, n // 4
    me = lax.axis_index("sp")
    outer, inner = lax.div(me, 2), lax.rem(me, 2)
    grp, mem = lax.div(outer, 2), lax.rem(outer, 2)
    opp, omem = 1 - inner, 1 - mem
    mate = outer * 2 + opp
    pair = (grp * 2 + omem) * 2 + inner
    cross = (grp * 2 + omem) * 2 + opp
    tme = lax.axis_index("tp")
    touter, tinner = lax.div(tme, 2), lax.rem(tme, 2)
    tmate = touter * 2 + (1 - tinner)
    kr, channels = wq_ref.shape
    kvc = wk_any.shape[0 if flip else 1]
    width = x_ref.shape[1]
    half = channels // 2
    quarter = width // nt
    heads = half // head_dim
    taps = cw_ref.shape[0]
    gp = 4 * span

    def rows_of(i, size):
        return pl.ds(pl.multiple_of(i * size, size), size)

    def partner(d):
        who, bit = 0, 1
        while bit < no:
            own = lax.rem(lax.div(outer, bit), 2)
            who = who + bit * (1 - own if d & bit else own)
            bit *= 2
        return who

    def copy(src, dst, send, recv, **where):
        return pltpu.make_async_remote_copy(
            src_ref=src, dst_ref=dst, send_sem=send, recv_sem=recv, device_id=where, device_id_type=MESH
        )

    out_cols = rows_of(tme, out_ref.shape[1])
    staged = [
        pltpu.make_async_copy(src, dst, loads.at[i])
        for i, (src, dst) in enumerate((
            (x_any, x_ref), (norm_any, norm_ref), (wk_any, kvsrc.at[0]), (wv_any, kvsrc.at[1]), (wr_any, wr_ref), (wq_any, wq_ref),
            (wg_any, wg_ref), (de_any, de_ref), (oa_any.at[:, out_cols], wall.at[0, tme]), (or_any.at[:, out_cols], wall.at[1, tme]),
            (qg_any, qg_ref), (kg_any, kg_ref), (fc_any, fc_ref), (cw_any, cw_ref), (dgw_any, dgw_ref),
            (igw_any, igw_ref), (dp_any, dp_ref), (ag_any, ag_ref), (rg_any, rg_ref),
        ))
    ]
    for load in staged:
        load.start()
    barrier = pltpu.get_barrier_semaphore()
    for d in range(1, n):
        pl.semaphore_signal(barrier, inc=1, device_id={"sp": lax.rem(me + d, n)}, device_id_type=MESH)
    for d in range(1, nt):
        pl.semaphore_signal(barrier, inc=1, device_id={"tp": lax.rem(tme + d, nt)}, device_id_type=MESH)

    mine_block, mate_block = mem * 2 + inner, mem * 2 + opp
    pair_block, cross_block = omem * 2 + inner, omem * 2 + opp
    my_half, my_rows = rows_of(mem, half), rows_of(me, kr)
    my_cols = rows_of(tme, quarter)

    staged[0].wait()
    staged[1].wait()

    def scale_rows(seq):
        x = x_ref[rows_of(seq, span), :].astype(F32)
        return lax.rsqrt(jnp.mean(x * x, axis=-1, keepdims=True) + EPS)

    xsend[...] = (
        x_ref[rows_of(opp, span), my_cols].astype(F32) * scale_rows(opp) * norm_ref[:, my_cols]
    ).astype(BF16)
    xall[mine_block] = (x_ref[rows_of(inner, span), :].astype(F32) * scale_rows(inner) * norm_ref[...]).astype(BF16)
    for load in staged[2:]:
        load.wait()
    pl.semaphore_wait(barrier, n - 1 + nt - 1)

    weights = (None, wr_ref, wq_ref, wg_ref)
    buffers = (kvw, rw, qw, gw)

    def place(c, who):
        return kvw.at[:, rows_of(who, kr)] if c == 0 and flip else buffers[c].at[rows_of(who, kr), :]

    def origin(c, member):
        return kvsrc.at[member] if c == 0 else weights[c].at[:, rows_of(member, half)]

    def outward(c, d):
        to = partner(d)
        return copy(origin(c, lax.rem(to, 2)), place(c, me), zs.at[c], zr.at[c, d - 1], sp=to * 2 + inner)

    def inward(c, d):
        who = partner(d) * 2 + inner
        return copy(place(c, who), place(c, who), zs.at[c], zr.at[c, d - 1], sp=mate)

    def across(c, d, who, src=None):
        return copy(place(c, who) if src is None else src, place(c, who), zs.at[c], fr.at[c], sp=mate)

    line = no == 4
    middle = (outer == 1) | (outer == 2)

    def send_z(c, which=range(1, no)):
        for d in which:
            if line and c > 0 and d == no - 1:
                pl.when(jnp.logical_not(middle))(outward(c, d).start)
            else:
                outward(c, d).start()

    def send_y(c):
        across(c, 0, me, origin(c, mem)).start()

    def forward(c, which=range(1, no)):
        for d in which:
            inward(c, d).wait_recv()
            across(c, d, partner(d) * 2 + inner).start()

    def span_of(c, parts):
        return kvw.at[:, pl.ds(0, parts * kr)] if c == 0 and flip else buffers[c].at[pl.ds(0, parts * kr), :]

    def finish(c):
        copy(span_of(c, no), span_of(c, no), zs.at[c], fr.at[c], sp=mate).wait_recv()

    def drain(c):
        copy(span_of(c, n - 1), span_of(c, n - 1), zs.at[c], fr.at[c], sp=mate).wait_send()

    def piece_of(block, who=None):
        return xall.at[block, :, my_cols if who is None else rows_of(who, quarter)]

    to_mate_x = copy(xsend, piece_of(mine_block), xs, xar, sp=mate)
    to_pair_x = [
        copy(piece_of(mine_block), piece_of(mine_block), xs, xbr.at[0], sp=pair),
        copy(piece_of(mate_block), piece_of(mate_block), xs, xbr.at[1], sp=pair),
    ]
    shared = (mate_block, pair_block, cross_block)

    def to_far_x(k, d):
        far = lax.rem(touter + d, nto) * 2 + tinner
        return copy(piece_of(shared[k]), piece_of(shared[k]), xs, xcr.at[k, d - 1], tp=far)

    def to_core_x(k, d):
        ref = piece_of(shared[k], lax.rem(touter + nto - d, nto) * 2 + tinner)
        return copy(ref, ref, xs, xdr, tp=tmate)

    def spread(k):
        for d in range(1, nto):
            to_far_x(k, d).start()
        to_core_x(k, 0).start()

    def extra(i):
        to, seq, member = ((mate, opp, mem), (pair, inner, omem), (cross, opp, omem))[i]
        src = de_ref.at[rows_of(seq, span), rows_of(member, half)]
        return copy(src, deg.at[mine_block], des, der, sp=to)

    def out_weights(a, d):
        to = lax.rem(tme + d, nt)
        src = (oa_any, or_any)[a].at[:, rows_of(to, out_ref.shape[1])]
        return copy(src, wall.at[a, tme], ws, wr, tp=to)

    to_mate_x.start()
    to_pair_x[0].start()
    send_z(0)
    if line:
        for c in range(1, 4):
            pl.when(middle)(outward(c, no - 1).start)
    deg[mine_block] = de_ref[rows_of(inner, span), my_half]
    if flip:
        kvw[:, my_rows] = kvsrc[mem]
    else:
        kvw[my_rows, :] = kvsrc[mem]
    rw[my_rows, :] = wr_ref[:, my_half]
    qw[my_rows, :] = wq_ref[:, my_half]
    gw[my_rows, :] = wg_ref[:, my_half]

    to_mate_x.wait_recv()
    to_pair_x[1].start()
    spread(0)
    send_y(0)
    send_y(1)
    to_pair_x[0].wait_recv()
    spread(1)
    forward(0, (1,))
    send_y(2)
    send_y(3)
    to_pair_x[1].wait_recv()
    spread(2)
    for a in range(2):
        for d in range(1, nt):
            out_weights(a, d).start()
    send_z(1)
    send_z(2)
    forward(0, range(2, no))
    forward(1, (1,))
    for i in range(3):
        extra(i).start()
    forward(1, range(2, no - 1))
    for k in range(3):
        for d in range(1, nto):
            to_far_x(k, d).wait_recv()
            to_core_x(k, d).start()
    forward(1, (no - 1,))
    shares = xall.at[pl.ds(0, 3), :, pl.ds(0, nto * quarter)]
    copy(shares, shares, xs, xdr, tp=tmate).wait_recv()
    finish(0)

    def normed():
        return xall[...].reshape(gp, width)

    kv = lax.dot_general(normed(), kvw[...], (((1,), (1 if flip else 0,)), ((), ())), preferred_element_type=F32)
    kv = jnp.where(mem == 0, group_rms(kv, head_dim) * kg_ref[...], kv).astype(BF16)
    kv_all[mem, grp] = jnp.concatenate([kv[: gp // 2], kv[gp // 2 :]], axis=1)

    def kv_copy(d, who):
        to, ref = lax.rem(grp + d, ng) * 4 + mem * 2 + inner, kv_all.at[mem, who]
        return copy(ref, ref, kvs.at[d - 1], kvr.at[d - 1], sp=to)

    def kv_pair(d, member, who):
        ref = kv_all.at[member, who]
        return copy(ref, ref, kps.at[d], kpr.at[d], sp=pair)

    def state_copy(d, who):
        to = lax.rem(grp + d, ng) * 4 + mem * 2 + inner
        return copy(st_all.at[who], st_all.at[who], ss.at[d - 1], sr.at[d - 1], sp=to)

    def later(make, act_on):
        for d in range(1, ng):
            @pl.when(grp + d < ng)
            def _(d=d):
                act_on(make(d, grp))

    def earlier(make):
        for d in range(1, ng):
            @pl.when(grp >= d)
            def _(d=d):
                make(d, lax.rem(grp + ng - d, ng)).wait_recv()

    kv_pair(0, mem, grp).start()
    later(kv_copy, lambda c: c.start())
    send_z(3, (1,))
    forward(2, range(1, no - 1))

    finish(1)
    rec = dot(normed(), rw[...]).astype(BF16).astype(F32)
    rin[pl.ds(8, gp), :] = rec
    halo[0] = rec[gp - 8 : gp]
    halo[1] = jnp.zeros_like(halo[1])
    halo_copy = copy(halo.at[0], halo.at[2], hs, hr, sp=lax.rem(grp + 1, ng) * 4 + mem * 2 + inner)

    @pl.when(grp + 1 < ng)
    def _():
        halo_copy.start()

    send_z(3, range(2, no))
    lb = dgw_ref.shape[1]

    def recur():
        copy(deg.at[pl.ds(0, 3)], deg.at[pl.ds(0, 3)], des, der, sp=mate).wait_recv()
        rin[pl.ds(0, 8), :] = halo[1]
        cw = cw_ref[:, my_half].astype(F32)
        conv = jnp.zeros((gp, half), F32)
        for tap in range(taps):
            conv = conv + rin[pl.ds(8 - (taps - 1) + tap, gp), :] * cw[tap : tap + 1]
        conv = conv.astype(BF16)
        nb = half // lb
        gate_decay = jnp.concatenate([dot(conv[:, i * lb : (i + 1) * lb], dgw_ref[mem * nb + i]) for i in range(nb)], axis=1)
        gate_input = jnp.concatenate([dot(conv[:, i * lb : (i + 1) * lb], igw_ref[mem * nb + i]) for i in range(nb)], axis=1)
        log_decay = -LRU_CONST * sigmoid(gate_decay) * softplus(-dp_ref[:, my_half]) + deg[...].reshape(gp, half)
        state = jnp.sqrt(one_minus_exp(2.0 * log_decay)) * sigmoid(gate_input) * conv.astype(F32)
        decay = jnp.exp(log_decay)
        time = lax.broadcasted_iota(jnp.int32, state.shape, 0)
        shift = 1
        while shift < gp:
            if shift < 8:
                seen = time >= shift
                state = state + decay * jnp.where(seen, pltpu.roll(state, shift, 0), 0.0)
                decay = decay * jnp.where(seen, pltpu.roll(decay, shift, 0), 1.0)
            else:
                moved = state[shift:] + decay[shift:] * state[: gp - shift]
                faded = decay[shift:] * decay[: gp - shift]
                state = jnp.concatenate([state[:shift], moved], axis=0)
                decay = jnp.concatenate([decay[:shift], faded], axis=0)
            shift *= 2
        scanned[0] = decay
        scanned[1] = state
        st_all[grp, pl.ds(0, 1), :] = decay[gp - 1 : gp]
        st_all[grp, pl.ds(1, 1), :] = state[gp - 1 : gp]
        later(state_copy, lambda c: c.start())

    forward(2, (no - 1,))
    for d in range(1, ng):
        @pl.when(grp >= d)
        def _(d=d):
            who = lax.rem(grp + ng - d, ng)
            kv_copy(d, who).wait_recv()
            kv_pair(d, mem, who).start()

    early = (grp > 0) & (mem == 0)
    late = (grp > 0) & (mem > 0)
    @pl.when(early)
    def _():
        forward(3, (1,))

    @pl.when(grp > 0)
    def _():
        halo_copy.wait_recv()
        halo[1] = halo[2]

    recur()
    @pl.when(grp == 0)
    def _():
        forward(3, (1,))

    finish(2)
    scaling = head_dim ** (-0.5)
    query = dot(normed(), qw[...])
    gains = jnp.concatenate([qg_ref[...]] * heads, axis=1)
    query = ((group_rms(query, head_dim) * gains).astype(BF16) * scaling).astype(BF16)

    @pl.when(late)
    def _():
        forward(3, (1,))

    forward(3, range(2, no))
    kv_pair(0, omem, grp).wait_recv()
    def attend(carried, q, kb, vb, fade_row, mask):
        top, total, accum = carried
        s = lax.dot_general(q, kb, (((1,), (1,)), ((), ())), preferred_element_type=F32) - fade_row
        if mask is not None:
            s = jnp.where(mask, s, -jnp.inf)
        new_top = jnp.maximum(top, jnp.max(s, axis=-1, keepdims=True))
        w = jnp.exp(s - new_top)
        fade = jnp.exp(top - new_top)
        total = total * fade + jnp.sum(w, axis=-1, keepdims=True)
        return new_top, total, accum * fade + dot(w.astype(BF16), vb)

    qb = gp // 2
    jobs = [(h, i) for h in range(heads) for i in range(2)]

    def heads_of(which, j):
        packed = kv_all[which, j]
        return jnp.concatenate([packed[:, :kvc], packed[:, kvc:]], axis=0)

    def keys_of(j):
        k = heads_of(0, j)
        zero = jnp.zeros_like(k)
        return [jnp.concatenate([k if x == h else zero for x in range(heads)], axis=1) for h in range(heads)]

    k_own, v_own = keys_of(grp), heads_of(1, grp)
    carried = []
    for h, i in jobs:
        size = (i + 1) * qb
        kb, vb = k_own[h][:size], v_own[:size]
        fade_row = fc_ref[inner, pl.ds(mem * heads + h, 1), pl.ds(pl.multiple_of(grp * gp, gp), size)]
        mask = i * qb + lax.broadcasted_iota(jnp.int32, (qb, size), 0) >= lax.broadcasted_iota(jnp.int32, (qb, size), 1)
        start = (jnp.full((qb, 1), -1e30, F32), jnp.zeros((qb, 1), F32), jnp.zeros((qb, head_dim), F32))
        carried.append(attend(start, query[i * qb : size], kb, vb, fade_row, mask))

    for d in range(1, ng):
        @pl.when(grp >= d)
        def _(d=d):
            kv_pair(d, omem, lax.rem(grp + ng - d, ng)).wait_recv()

    def step(j, carried):
        result = []
        keys, vb = keys_of(j), heads_of(1, j)
        for (h, i), state_of in zip(jobs, carried):
            fade_row = fc_ref[inner, pl.ds(mem * heads + h, 1), pl.ds(pl.multiple_of(j * gp, gp), gp)]
            result.append(attend(state_of, query[i * qb : (i + 1) * qb], keys[h], vb, fade_row, None))
        return tuple(result)

    carried = lax.fori_loop(0, grp, step, tuple(carried))
    columns = []
    for h in range(heads):
        columns.append(jnp.concatenate([c[2] * (1.0 / c[1]) for (hh, i), c in zip(jobs, carried) if hh == h], axis=0))
    attended = group_rms(jnp.concatenate(columns, axis=1), head_dim) * ag_ref[:, my_half]

    def act_copy(a, i):
        to, block = ((mate, mate_block), (pair, pair_block), (cross, cross_block))[i]
        return copy(
            act.at[a, block], gath.at[a, tme, rows_of(inner, span), my_half], acs, acr.at[a], sp=to
        )

    def act_from(a):
        copy(act.at[a, pl.ds(0, 3)], act.at[a, pl.ds(0, 3)], acs, acr.at[a], sp=mate).wait_recv()

    def hand_out(a, values):
        act[a] = values.astype(BF16).reshape(4, span, half)
        for i in range(3):
            act_copy(a, i).start()
        gath[a, tme, rows_of(inner, span), my_half] = act[a, mine_block]

    hand_out(0, attended)

    earlier(state_copy)

    def enter(j, e):
        return st_all[j, pl.ds(0, 1), :] * e + st_all[j, pl.ds(1, 1), :]

    entering = lax.fori_loop(0, grp, enter, jnp.zeros((1, half), F32))
    whole_state = scanned[1] + scanned[0] * entering
    def far_of(d):
        return lax.rem(touter + nto + d, nto) * 2

    def to_far(a, d):
        return copy(gath.at[a, tme], gath.at[a, tme], ps, qr.at[a, d - 1], tp=far_of(d) + tinner)

    def to_core(a, d):
        ref = gath.at[a, far_of(-d) + tinner]
        return copy(ref, ref, ps, pr.at[a, d], tp=tmate)

    def gather(a):
        act_from(a)
        for d in range(1, nto):
            to_far(a, d).start()
        to_core(a, 0).start()

    def relay(a):
        for d in range(1, nto):
            ref = gath.at[a, far_of(-d) + tinner]
            copy(ref, ref, ps, qr.at[a, d - 1], tp=tmate).wait_recv()
            to_core(a, d).start()

    def arrive(a, d):
        ref = gath.at[a, far_of(-d) + 1 - tinner]
        copy(ref, ref, ps, pr.at[a, d], tp=tmate).wait_recv()

    def term(a, who):
        return dot(gath[a, who], wall[a, who])

    finish(3)
    gated = whole_state * gelu(dot(normed(), gw[...]))

    hand_out(1, group_rms(gated, lb) * rg_ref[:, my_half])
    gather(0)
    gather(1)
    relay(0)
    copy(wall.at[:, pl.ds(0, nt - 1)], wall.at[:, pl.ds(0, nt - 1)], ws, wr, tp=tmate).wait_recv()
    acc[...] = term(0, tme)
    for d in range(nto):
        arrive(0, d)
        acc[...] += term(0, far_of(-d) + 1 - tinner)
        if d:
            acc[...] += term(0, far_of(-d) + tinner)
    acc[...] += term(1, tme)
    relay(1)
    for d in range(1, nto):
        acc[...] += term(1, far_of(-d) + tinner)
    arrive(1, 0)
    acc[...] += term(1, tmate)
    for d in range(1, nto):
        arrive(1, d)
        acc[...] += term(1, far_of(-d) + 1 - tinner)
    out_ref[...] = acc[...].astype(BF16)
    for c in range(4):
        drain(c)
    copy(xall.at[pl.ds(0, 3)], xall.at[pl.ds(0, 3)], xs, xar, sp=mate).wait_send()
    copy(deg.at[pl.ds(0, 3)], deg.at[pl.ds(0, 3)], des, der, sp=mate).wait_send()
    later(kv_copy, lambda c: c.wait_send())
    kv_pair(0, mem, grp).wait_send()
    for d in range(1, ng):
        @pl.when(grp >= d)
        def _(d=d):
            kv_pair(d, mem, lax.rem(grp + ng - d, ng)).wait_send()

    later(state_copy, lambda c: c.wait_send())

    @pl.when(grp + 1 < ng)
    def _():
        halo_copy.wait_send()

    copy(act.at[:, pl.ds(0, 3)], act.at[:, pl.ds(0, 3)], acs, acr.at[0], sp=mate).wait_send()
    copy(wall.at[:, pl.ds(0, nt - 1)], wall.at[:, pl.ds(0, nt - 1)], ws, wr, tp=tmate).wait_send()
    copy(gath.at[:, pl.ds(0, nt - 1)], gath.at[:, pl.ds(0, nt - 1)], ps, wr, tp=tmate).wait_send()


def body(
    n, nt,
    inputs, norm_gain, query_weight, key_weight, value_weight, query_gain, key_gain, forget_cache,
    rec_in_weight, rec_gate_weight, conv_weight, decay_gate_weight, input_gate_weight, decay_param,
    decay_extra, attn_out_gain, rec_out_gain, out_att_weight, out_rec_weight,
):
    seqs, span, width = inputs.shape
    assert seqs == 2 and n % 4 == 0 and nt % 2 == 0 and key_weight.shape[1] == query_gain.shape[0]
    rows = seqs * span
    head_dim = query_gain.shape[0]
    channels = rec_in_weight.shape[1]
    qc, kvc = query_weight.shape[1], key_weight.shape[1]
    half = channels // 2
    cols = out_att_weight.shape[1] // nt
    flip = query_weight.shape[0] % 128 == 0
    kv_weights = [w.T if flip else w for w in (key_weight, value_weight)]
    no, nto, ng = n // 2, nt // 2, n // 4
    dma = pltpu.SemaphoreType.DMA
    vmem, far = pl.BlockSpec(memory_space=pltpu.VMEM), pl.BlockSpec(memory_space=pltpu.HBM)
    out = pl.pallas_call(
        functools.partial(kernel, (n, nt, span, head_dim, flip)),
        out_shape=pltpu.VMEM((rows, cols), BF16),
        in_specs=[far] * 19,
        out_specs=vmem,
        scratch_shapes=[
            pltpu.VMEM((rows, width), BF16),
            pltpu.VMEM(query_weight.shape, BF16),
            pltpu.VMEM(rec_in_weight.shape, BF16),
            pltpu.VMEM(rec_gate_weight.shape, BF16),
            pltpu.VMEM((rows, channels), F32),
            pltpu.VMEM((2, nt, channels, cols), BF16),
            pltpu.VMEM((1, width), F32),
            pltpu.VMEM((1, head_dim), F32),
            pltpu.VMEM((1, head_dim), F32),
            pltpu.VMEM(forget_cache.shape, F32),
            pltpu.VMEM(conv_weight.shape, BF16),
            pltpu.VMEM(decay_gate_weight.shape, BF16),
            pltpu.VMEM(input_gate_weight.shape, BF16),
            pltpu.VMEM((1, channels), F32),
            pltpu.VMEM((1, qc), F32),
            pltpu.VMEM((1, channels), F32),
            dma((19,)),
            pltpu.VMEM((4, span, width), BF16),
            pltpu.VMEM((span, width // nt), BF16),
            pltpu.VMEM((2, *kv_weights[0].shape), BF16),
            pltpu.VMEM((kvc, width) if flip else (width, kvc), BF16),
            pltpu.VMEM((width, half), BF16),
            pltpu.VMEM((width, half), BF16),
            pltpu.VMEM((width, half), BF16),
            pltpu.VMEM((2, ng, 2 * span, 2 * kvc), BF16),
            pltpu.VMEM((2, 4 * span, half), F32),
            pltpu.VMEM((4, span, half), F32),
            pltpu.VMEM((4 * span + 8, half), F32),
            pltpu.VMEM((3, 8, half), F32),
            pltpu.VMEM((ng, 8, half), F32),
            pltpu.VMEM((2, 4, span, half), BF16),
            pltpu.VMEM((2, nt, rows, channels), BF16),
            pltpu.VMEM((rows, cols), F32),
            dma((4,)), dma((4, no - 1)), dma((4,)), dma, dma, dma((2,)), dma((3, nto - 1)), dma,
            dma, dma, dma((ng - 1,)), dma((ng - 1,)), dma((ng,)), dma((ng,)), dma, dma, dma((ng - 1,)), dma((ng - 1,)),
            dma, dma((2,)), dma, dma((2, nto)), dma((2, nto - 1)), dma, dma,
        ],
        compiler_params=pltpu.CompilerParams(
            collective_id=0, has_side_effects=True, vmem_limit_bytes=60 * 1024 * 1024
        ),
    )(
        inputs.reshape(rows, width), norm_gain.reshape(1, width), query_weight, *kv_weights,
        query_gain.reshape(1, head_dim), key_gain.reshape(1, head_dim), forget_cache,
        rec_in_weight, rec_gate_weight, conv_weight, decay_gate_weight, input_gate_weight,
        decay_param.reshape(1, channels), decay_extra.reshape(rows, channels),
        attn_out_gain.reshape(1, qc), rec_out_gain.reshape(1, channels), out_att_weight, out_rec_weight,
    )
    return out.reshape(seqs, span, cols)


def solution(mesh):
    return jax.shard_map(
        functools.partial(body, mesh.shape["sp"], mesh.shape["tp"]),
        mesh=mesh,
        in_specs=(
            P(None, "sp", None), P(), P("sp", "tp"), P("sp", "tp"), P("sp", "tp"), P(), P(),
            P(None, "tp", None), P("sp", "tp"), P("sp", "tp"), P(None, "tp"), P("tp", None, None),
            P("tp", None, None), P("tp"), P(None, "sp", "tp"), P("tp"), P("tp"), P("tp", None), P("tp", None),
        ),
        out_specs=P(None, "sp", "tp"),
        check_vma=False,
    )
```

```python
import functools

import jax
import jax.numpy as jnp
from jax import lax
from jax.experimental import pallas as pl
from jax.experimental.pallas import tpu as pltpu
from jax.sharding import PartitionSpec as P

LRU_CONST = 8.0
EPS = 1e-06
F32 = jnp.float32
BF16 = jnp.bfloat16
MESH = pl.DeviceIdType.MESH


def group_rms(values, width):
    lane = lax.broadcasted_iota(jnp.int32, values.shape, 1)
    squares, scale = values * values, 0.0
    for start in range(0, values.shape[1], width):
        inside = (lane >= start) & (lane < start + width)
        mean = jnp.sum(jnp.where(inside, squares, 0.0), axis=-1, keepdims=True) * (1.0 / width)
        scale = jnp.where(inside, lax.rsqrt(mean + EPS), scale)
    return values * scale


def one_minus_exp(y):
    series = y * (1 + y / 2 * (1 + y / 3 * (1 + y / 4 * (1 + y / 5 * (1 + y / 6 * (1 + y / 7))))))
    return -jnp.where(y > -0.4, series, jnp.exp(y) - 1.0)


def softplus(x):
    u = jnp.exp(-jnp.abs(x))
    s = u / (2.0 + u)
    q = s * s
    series = 1.0 / 17
    for odd in (15, 13, 11, 9, 7, 5, 3, 1):
        series = series * q + 1.0 / odd
    return jnp.maximum(x, 0.0) + 2.0 * s * series


def sigmoid(x):
    return 1.0 / (1.0 + jnp.exp(-x))


def gelu(x):
    return 0.5 * x * (1.0 + jnp.tanh(0.7978845608028654 * (x + 0.044715 * x * x * x)))


def dot(a, b):
    return jnp.dot(a, b, preferred_element_type=F32)


def kernel(
    dims,
    x_any, norm_any, wq_any, wk_any, wv_any, qg_any, kg_any, fc_any, wr_any, wg_any, cw_any,
    dgw_any, igw_any, dp_any, de_any, ag_any, rg_any, oa_any, or_any,
    out_ref,
    x_ref, wq_ref, wr_ref, wg_ref, de_ref, wall, norm_ref, qg_ref, kg_ref, fc_ref, cw_ref, dgw_ref, igw_ref, dp_ref,
    ag_ref, rg_ref, loads, xall, xsend, kvsrc, kvw, rw, qw, gw, kv_all, scanned, deg, rin, halo, st_all, act, gath, acc,
    zs, zr, fr, xs, xar, xbr, xcr, xdr, des, der, kvs, kvr, kps, kpr, hs, hr, ss, sr,
    acs, acr, ps, pr, qr, ws, wr,
):
    n, nt, span, head_dim, flip = dims
    no, nto, ng = n // 2, nt // 2, n // 4
    me = lax.axis_index("sp")
    outer, inner = lax.div(me, 2), lax.rem(me, 2)
    grp, mem = lax.div(outer, 2), lax.rem(outer, 2)
    opp, omem = 1 - inner, 1 - mem
    mate = outer * 2 + opp
    pair = (grp * 2 + omem) * 2 + inner
    cross = (grp * 2 + omem) * 2 + opp
    tme = lax.axis_index("tp")
    touter, tinner = lax.div(tme, 2), lax.rem(tme, 2)
    tmate = touter * 2 + (1 - tinner)
    kr, channels = wq_ref.shape
    kvc = wk_any.shape[0 if flip else 1]
    width = x_ref.shape[1]
    half = channels // 2
    quarter = width // nt
    heads = half // head_dim
    taps = cw_ref.shape[0]
    gp = 4 * span

    def rows_of(i, size):
        return pl.ds(pl.multiple_of(i * size, size), size)

    def partner(d):
        who, bit = 0, 1
        while bit < no:
            own = lax.rem(lax.div(outer, bit), 2)
            who = who + bit * (1 - own if d & bit else own)
            bit *= 2
        return who

    def copy(src, dst, send, recv, **where):
        return pltpu.make_async_remote_copy(
            src_ref=src, dst_ref=dst, send_sem=send, recv_sem=recv, device_id=where, device_id_type=MESH
        )

    out_cols = rows_of(tme, out_ref.shape[1])
    staged = [
        pltpu.make_async_copy(src, dst, loads.at[i])
        for i, (src, dst) in enumerate((
            (x_any, x_ref), (norm_any, norm_ref), (wk_any, kvsrc.at[0]), (wv_any, kvsrc.at[1]), (wr_any, wr_ref), (wq_any, wq_ref),
            (wg_any, wg_ref), (de_any, de_ref), (oa_any.at[:, out_cols], wall.at[0, tme]), (or_any.at[:, out_cols], wall.at[1, tme]),
            (qg_any, qg_ref), (kg_any, kg_ref), (fc_any, fc_ref), (cw_any, cw_ref), (dgw_any, dgw_ref),
            (igw_any, igw_ref), (dp_any, dp_ref), (ag_any, ag_ref), (rg_any, rg_ref),
        ))
    ]
    for load in staged:
        load.start()
    barrier = pltpu.get_barrier_semaphore()
    for d in range(1, n):
        pl.semaphore_signal(barrier, inc=1, device_id={"sp": lax.rem(me + d, n)}, device_id_type=MESH)
    for d in range(1, nt):
        pl.semaphore_signal(barrier, inc=1, device_id={"tp": lax.rem(tme + d, nt)}, device_id_type=MESH)

    mine_block, mate_block = mem * 2 + inner, mem * 2 + opp
    pair_block, cross_block = omem * 2 + inner, omem * 2 + opp
    my_half, my_rows = rows_of(mem, half), rows_of(me, kr)
    my_cols = rows_of(tme, quarter)

    staged[0].wait()
    staged[1].wait()

    def scale_rows(seq):
        x = x_ref[rows_of(seq, span), :].astype(F32)
        return lax.rsqrt(jnp.mean(x * x, axis=-1, keepdims=True) + EPS)

    xsend[...] = (
        x_ref[rows_of(opp, span), my_cols].astype(F32) * scale_rows(opp) * norm_ref[:, my_cols]
    ).astype(BF16)
    xall[mine_block] = (x_ref[rows_of(inner, span), :].astype(F32) * scale_rows(inner) * norm_ref[...]).astype(BF16)
    for load in staged[2:]:
        load.wait()
    pl.semaphore_wait(barrier, n - 1 + nt - 1)

    weights = (None, wr_ref, wq_ref, wg_ref)
    buffers = (kvw, rw, qw, gw)

    def place(c, who):
        return kvw.at[:, rows_of(who, kr)] if c == 0 and flip else buffers[c].at[rows_of(who, kr), :]

    def origin(c, member):
        return kvsrc.at[member] if c == 0 else weights[c].at[:, rows_of(member, half)]

    def outward(c, d):
        to = partner(d)
        return copy(origin(c, lax.rem(to, 2)), place(c, me), zs.at[c], zr.at[c, d - 1], sp=to * 2 + inner)

    def inward(c, d):
        who = partner(d) * 2 + inner
        return copy(place(c, who), place(c, who), zs.at[c], zr.at[c, d - 1], sp=mate)

    def across(c, d, who, src=None):
        return copy(place(c, who) if src is None else src, place(c, who), zs.at[c], fr.at[c], sp=mate)

    line = no == 4
    middle = (outer == 1) | (outer == 2)

    def send_z(c, which=range(1, no)):
        for d in which:
            if line and c > 0 and d == no - 1:
                pl.when(jnp.logical_not(middle))(outward(c, d).start)
            else:
                outward(c, d).start()

    def send_y(c):
        across(c, 0, me, origin(c, mem)).start()

    def forward(c, which=range(1, no)):
        for d in which:
            inward(c, d).wait_recv()
            across(c, d, partner(d) * 2 + inner).start()

    def span_of(c, parts):
        return kvw.at[:, pl.ds(0, parts * kr)] if c == 0 and flip else buffers[c].at[pl.ds(0, parts * kr), :]

    def finish(c):
        copy(span_of(c, no), span_of(c, no), zs.at[c], fr.at[c], sp=mate).wait_recv()

    def drain(c):
        copy(span_of(c, n - 1), span_of(c, n - 1), zs.at[c], fr.at[c], sp=mate).wait_send()

    def piece_of(block, who=None):
        return xall.at[block, :, my_cols if who is None else rows_of(who, quarter)]

    to_mate_x = copy(xsend, piece_of(mine_block), xs, xar, sp=mate)
    to_pair_x = [
        copy(piece_of(mine_block), piece_of(mine_block), xs, xbr.at[0], sp=pair),
        copy(piece_of(mate_block), piece_of(mate_block), xs, xbr.at[1], sp=pair),
    ]
    shared = (mate_block, pair_block, cross_block)

    def to_far_x(k, d):
        far = lax.rem(touter + d, nto) * 2 + tinner
        return copy(piece_of(shared[k]), piece_of(shared[k]), xs, xcr.at[k, d - 1], tp=far)

    def to_core_x(k, d):
        ref = piece_of(shared[k], lax.rem(touter + nto - d, nto) * 2 + tinner)
        return copy(ref, ref, xs, xdr, tp=tmate)

    def spread(k):
        for d in range(1, nto):
            to_far_x(k, d).start()
        to_core_x(k, 0).start()

    def extra(i):
        to, seq, member = ((mate, opp, mem), (pair, inner, omem), (cross, opp, omem))[i]
        src = de_ref.at[rows_of(seq, span), rows_of(member, half)]
        return copy(src, deg.at[mine_block], des, der, sp=to)

    def out_weights(a, d):
        to = lax.rem(tme + d, nt)
        src = (oa_any, or_any)[a].at[:, rows_of(to, out_ref.shape[1])]
        return copy(src, wall.at[a, tme], ws, wr, tp=to)

    to_mate_x.start()
    to_pair_x[0].start()
    send_z(0)
    if line:
        for c in range(1, 4):
            pl.when(middle)(outward(c, no - 1).start)
    deg[mine_block] = de_ref[rows_of(inner, span), my_half]
    if flip:
        kvw[:, my_rows] = kvsrc[mem]
    else:
        kvw[my_rows, :] = kvsrc[mem]
    rw[my_rows, :] = wr_ref[:, my_half]
    qw[my_rows, :] = wq_ref[:, my_half]
    gw[my_rows, :] = wg_ref[:, my_half]

    to_mate_x.wait_recv()
    to_pair_x[1].start()
    spread(0)
    send_y(0)
    send_y(1)
    to_pair_x[0].wait_recv()
    spread(1)
    forward(0, (1,))
    send_y(2)
    send_y(3)
    to_pair_x[1].wait_recv()
    spread(2)
    for a in range(2):
        for d in range(1, nt):
            out_weights(a, d).start()
    send_z(1)
    send_z(2)
    for i in range(3):
        extra(i).start()
    forward(0, range(2, no))
    forward(1, (1,))
    forward(1, range(2, no - 1))
    for k in range(3):
        for d in range(1, nto):
            to_far_x(k, d).wait_recv()
            to_core_x(k, d).start()
    forward(1, (no - 1,))
    shares = xall.at[pl.ds(0, 3), :, pl.ds(0, nto * quarter)]
    copy(shares, shares, xs, xdr, tp=tmate).wait_recv()
    finish(0)

    def normed():
        return xall[...].reshape(gp, width)

    kv = lax.dot_general(normed(), kvw[...], (((1,), (1 if flip else 0,)), ((), ())), preferred_element_type=F32)
    kv = jnp.where(mem == 0, group_rms(kv, head_dim) * kg_ref[...], kv).astype(BF16)
    kv_all[mem, grp] = jnp.concatenate([kv[: gp // 2], kv[gp // 2 :]], axis=1)

    def project_part(weights, line):
        total = 0.0
        for z in range(no):
            block = rows_of(z * 2 + line, kr)
            total = total + dot(xall[:, :, block].reshape(gp, kr), weights[block, :])
        return total

    def project(c):
        if not flip:
            finish(c)
            return dot(normed(), buffers[c][...])
        total = project_part(buffers[c], inner)
        finish(c)
        return total + project_part(buffers[c], opp)

    def kv_copy(d, who):
        to, ref = lax.rem(grp + d, ng) * 4 + mem * 2 + inner, kv_all.at[mem, who]
        return copy(ref, ref, kvs.at[d - 1], kvr.at[d - 1], sp=to)

    def kv_pair(d, member, who):
        ref = kv_all.at[member, who]
        return copy(ref, ref, kps.at[d], kpr.at[d], sp=pair)

    def state_copy(d, who):
        to = lax.rem(grp + d, ng) * 4 + mem * 2 + inner
        return copy(st_all.at[who], st_all.at[who], ss.at[d - 1], sr.at[d - 1], sp=to)

    def later(make, act_on):
        for d in range(1, ng):
            @pl.when(grp + d < ng)
            def _(d=d):
                act_on(make(d, grp))

    def earlier(make):
        for d in range(1, ng):
            @pl.when(grp >= d)
            def _(d=d):
                make(d, lax.rem(grp + ng - d, ng)).wait_recv()

    kv_pair(0, mem, grp).start()
    later(kv_copy, lambda c: c.start())
    send_z(3, (1,))
    forward(2, range(1, no - 1))

    rec = project(1).astype(BF16).astype(F32)
    rin[pl.ds(8, gp), :] = rec
    halo[0] = rec[gp - 8 : gp]
    halo[1] = jnp.zeros_like(halo[1])
    halo_copy = copy(halo.at[0], halo.at[2], hs, hr, sp=lax.rem(grp + 1, ng) * 4 + mem * 2 + inner)

    @pl.when(grp + 1 < ng)
    def _():
        halo_copy.start()

    send_z(3, range(2, no))
    lb = dgw_ref.shape[1]

    def recur():
        copy(deg.at[pl.ds(0, 3)], deg.at[pl.ds(0, 3)], des, der, sp=mate).wait_recv()
        rin[pl.ds(0, 8), :] = halo[1]
        cw = cw_ref[:, my_half].astype(F32)
        conv = jnp.zeros((gp, half), F32)
        for tap in range(taps):
            conv = conv + rin[pl.ds(8 - (taps - 1) + tap, gp), :] * cw[tap : tap + 1]
        conv = conv.astype(BF16)
        nb = half // lb
        gate_decay = jnp.concatenate([dot(conv[:, i * lb : (i + 1) * lb], dgw_ref[mem * nb + i]) for i in range(nb)], axis=1)
        gate_input = jnp.concatenate([dot(conv[:, i * lb : (i + 1) * lb], igw_ref[mem * nb + i]) for i in range(nb)], axis=1)
        log_decay = -LRU_CONST * sigmoid(gate_decay) * softplus(-dp_ref[:, my_half]) + deg[...].reshape(gp, half)
        state = jnp.sqrt(one_minus_exp(2.0 * log_decay)) * sigmoid(gate_input) * conv.astype(F32)
        decay = jnp.exp(log_decay)
        time = lax.broadcasted_iota(jnp.int32, state.shape, 0)
        shift = 1
        while shift < gp:
            if shift < 8:
                seen = time >= shift
                state = state + decay * jnp.where(seen, pltpu.roll(state, shift, 0), 0.0)
                decay = decay * jnp.where(seen, pltpu.roll(decay, shift, 0), 1.0)
            else:
                moved = state[shift:] + decay[shift:] * state[: gp - shift]
                faded = decay[shift:] * decay[: gp - shift]
                state = jnp.concatenate([state[:shift], moved], axis=0)
                decay = jnp.concatenate([decay[:shift], faded], axis=0)
            shift *= 2
        scanned[0] = decay
        scanned[1] = state
        st_all[grp, pl.ds(0, 1), :] = decay[gp - 1 : gp]
        st_all[grp, pl.ds(1, 1), :] = state[gp - 1 : gp]
        later(state_copy, lambda c: c.start())

    forward(2, (no - 1,))
    for d in range(1, ng):
        @pl.when(grp >= d)
        def _(d=d):
            who = lax.rem(grp + ng - d, ng)
            kv_copy(d, who).wait_recv()
            kv_pair(d, mem, who).start()

    early = (grp > 0) & (mem == 0)
    late = (grp > 0) & (mem > 0)
    @pl.when(early)
    def _():
        forward(3, (1,))

    @pl.when(grp > 0)
    def _():
        halo_copy.wait_recv()
        halo[1] = halo[2]

    recur()
    @pl.when(grp == 0)
    def _():
        forward(3, (1,))

    query = project(2)
    scaling = head_dim ** (-0.5)
    gains = jnp.concatenate([qg_ref[...]] * heads, axis=1)
    query = ((group_rms(query, head_dim) * gains).astype(BF16) * scaling).astype(BF16)

    @pl.when(late)
    def _():
        forward(3, (1,))

    forward(3, range(2, no))
    kv_pair(0, omem, grp).wait_recv()
    def attend(carried, q, kb, vb, fade_row, mask):
        top, total, accum = carried
        s = lax.dot_general(q, kb, (((1,), (1,)), ((), ())), preferred_element_type=F32) - fade_row
        if mask is not None:
            s = jnp.where(mask, s, -jnp.inf)
        new_top = jnp.maximum(top, jnp.max(s, axis=-1, keepdims=True))
        w = jnp.exp(s - new_top)
        fade = jnp.exp(top - new_top)
        total = total * fade + jnp.sum(w, axis=-1, keepdims=True)
        return new_top, total, accum * fade + dot(w.astype(BF16), vb)

    qb = gp // 2
    jobs = [(h, i) for h in range(heads) for i in range(2)]

    def heads_of(which, j):
        packed = kv_all[which, j]
        return jnp.concatenate([packed[:, :kvc], packed[:, kvc:]], axis=0)

    def keys_of(j):
        k = heads_of(0, j)
        zero = jnp.zeros_like(k)
        return [jnp.concatenate([k if x == h else zero for x in range(heads)], axis=1) for h in range(heads)]

    k_own, v_own = keys_of(grp), heads_of(1, grp)
    carried = []
    for h, i in jobs:
        size = (i + 1) * qb
        kb, vb = k_own[h][:size], v_own[:size]
        fade_row = fc_ref[inner, pl.ds(mem * heads + h, 1), pl.ds(pl.multiple_of(grp * gp, gp), size)]
        mask = i * qb + lax.broadcasted_iota(jnp.int32, (qb, size), 0) >= lax.broadcasted_iota(jnp.int32, (qb, size), 1)
        start = (jnp.full((qb, 1), -1e30, F32), jnp.zeros((qb, 1), F32), jnp.zeros((qb, head_dim), F32))
        carried.append(attend(start, query[i * qb : size], kb, vb, fade_row, mask))

    for d in range(1, ng):
        @pl.when(grp >= d)
        def _(d=d):
            kv_pair(d, omem, lax.rem(grp + ng - d, ng)).wait_recv()

    def step(j, carried):
        result = []
        keys, vb = keys_of(j), heads_of(1, j)
        for (h, i), state_of in zip(jobs, carried):
            fade_row = fc_ref[inner, pl.ds(mem * heads + h, 1), pl.ds(pl.multiple_of(j * gp, gp), gp)]
            result.append(attend(state_of, query[i * qb : (i + 1) * qb], keys[h], vb, fade_row, None))
        return tuple(result)

    carried = lax.fori_loop(0, grp, step, tuple(carried))
    columns = []
    for h in range(heads):
        columns.append(jnp.concatenate([c[2] * (1.0 / c[1]) for (hh, i), c in zip(jobs, carried) if hh == h], axis=0))
    attended = group_rms(jnp.concatenate(columns, axis=1), head_dim) * ag_ref[:, my_half]

    def act_copy(a, i):
        to, block = ((mate, mate_block), (pair, pair_block), (cross, cross_block))[i]
        return copy(
            act.at[a, block], gath.at[a, tme, rows_of(inner, span), my_half], acs, acr.at[a], sp=to
        )

    def act_from(a):
        copy(act.at[a, pl.ds(0, 3)], act.at[a, pl.ds(0, 3)], acs, acr.at[a], sp=mate).wait_recv()

    def hand_out(a, values):
        act[a] = values.astype(BF16).reshape(4, span, half)
        for i in range(3):
            act_copy(a, i).start()
        gath[a, tme, rows_of(inner, span), my_half] = act[a, mine_block]

    hand_out(0, attended)

    earlier(state_copy)

    def enter(j, e):
        return st_all[j, pl.ds(0, 1), :] * e + st_all[j, pl.ds(1, 1), :]

    entering = lax.fori_loop(0, grp, enter, jnp.zeros((1, half), F32))
    whole_state = scanned[1] + scanned[0] * entering
    def far_of(d):
        return lax.rem(touter + nto + d, nto) * 2

    def to_far(a, d):
        return copy(gath.at[a, tme], gath.at[a, tme], ps, qr.at[a, d - 1], tp=far_of(d) + tinner)

    def to_core(a, d):
        ref = gath.at[a, far_of(-d) + tinner]
        return copy(ref, ref, ps, pr.at[a, d], tp=tmate)

    def gather(a):
        act_from(a)
        for d in range(1, nto):
            to_far(a, d).start()
        to_core(a, 0).start()

    def relay(a):
        for d in range(1, nto):
            ref = gath.at[a, far_of(-d) + tinner]
            copy(ref, ref, ps, qr.at[a, d - 1], tp=tmate).wait_recv()
            to_core(a, d).start()

    def arrive(a, d):
        ref = gath.at[a, far_of(-d) + 1 - tinner]
        copy(ref, ref, ps, pr.at[a, d], tp=tmate).wait_recv()

    def term(a, who):
        return dot(gath[a, who], wall[a, who])

    gate_proj = project(3)
    gated = whole_state * gelu(gate_proj)

    hand_out(1, group_rms(gated, lb) * rg_ref[:, my_half])
    gather(0)
    gather(1)
    relay(0)
    copy(wall.at[:, pl.ds(0, nt - 1)], wall.at[:, pl.ds(0, nt - 1)], ws, wr, tp=tmate).wait_recv()
    acc[...] = term(0, tme) + term(1, tme)
    arrive(0, 0)
    acc[...] += term(0, tmate)
    for d in range(1, nto):
        acc[...] += term(0, far_of(-d) + tinner)
    relay(1)
    for d in range(1, nto):
        arrive(0, d)
        acc[...] += term(0, far_of(-d) + 1 - tinner)
    for d in range(1, nto):
        acc[...] += term(1, far_of(-d) + tinner)
    arrive(1, 0)
    acc[...] += term(1, tmate)
    for d in range(1, nto):
        arrive(1, d)
        acc[...] += term(1, far_of(-d) + 1 - tinner)
    out_ref[...] = acc[...].astype(BF16)
    for c in range(4):
        drain(c)
    copy(xall.at[pl.ds(0, 3)], xall.at[pl.ds(0, 3)], xs, xar, sp=mate).wait_send()
    copy(deg.at[pl.ds(0, 3)], deg.at[pl.ds(0, 3)], des, der, sp=mate).wait_send()
    later(kv_copy, lambda c: c.wait_send())
    kv_pair(0, mem, grp).wait_send()
    for d in range(1, ng):
        @pl.when(grp >= d)
        def _(d=d):
            kv_pair(d, mem, lax.rem(grp + ng - d, ng)).wait_send()

    later(state_copy, lambda c: c.wait_send())

    @pl.when(grp + 1 < ng)
    def _():
        halo_copy.wait_send()

    copy(act.at[:, pl.ds(0, 3)], act.at[:, pl.ds(0, 3)], acs, acr.at[0], sp=mate).wait_send()
    copy(wall.at[:, pl.ds(0, nt - 1)], wall.at[:, pl.ds(0, nt - 1)], ws, wr, tp=tmate).wait_send()
    copy(gath.at[:, pl.ds(0, nt - 1)], gath.at[:, pl.ds(0, nt - 1)], ps, wr, tp=tmate).wait_send()


def body(
    n, nt,
    inputs, norm_gain, query_weight, key_weight, value_weight, query_gain, key_gain, forget_cache,
    rec_in_weight, rec_gate_weight, conv_weight, decay_gate_weight, input_gate_weight, decay_param,
    decay_extra, attn_out_gain, rec_out_gain, out_att_weight, out_rec_weight,
):
    seqs, span, width = inputs.shape
    assert seqs == 2 and n % 4 == 0 and nt % 2 == 0 and key_weight.shape[1] == query_gain.shape[0]
    rows = seqs * span
    head_dim = query_gain.shape[0]
    channels = rec_in_weight.shape[1]
    qc, kvc = query_weight.shape[1], key_weight.shape[1]
    half = channels // 2
    cols = out_att_weight.shape[1] // nt
    flip = query_weight.shape[0] % 128 == 0
    kv_weights = [w.T if flip else w for w in (key_weight, value_weight)]
    no, nto, ng = n // 2, nt // 2, n // 4
    dma = pltpu.SemaphoreType.DMA
    vmem, far = pl.BlockSpec(memory_space=pltpu.VMEM), pl.BlockSpec(memory_space=pltpu.HBM)
    out = pl.pallas_call(
        functools.partial(kernel, (n, nt, span, head_dim, flip)),
        out_shape=pltpu.VMEM((rows, cols), BF16),
        in_specs=[far] * 19,
        out_specs=vmem,
        scratch_shapes=[
            pltpu.VMEM((rows, width), BF16),
            pltpu.VMEM(query_weight.shape, BF16),
            pltpu.VMEM(rec_in_weight.shape, BF16),
            pltpu.VMEM(rec_gate_weight.shape, BF16),
            pltpu.VMEM((rows, channels), F32),
            pltpu.VMEM((2, nt, channels, cols), BF16),
            pltpu.VMEM((1, width), F32),
            pltpu.VMEM((1, head_dim), F32),
            pltpu.VMEM((1, head_dim), F32),
            pltpu.VMEM(forget_cache.shape, F32),
            pltpu.VMEM(conv_weight.shape, BF16),
            pltpu.VMEM(decay_gate_weight.shape, BF16),
            pltpu.VMEM(input_gate_weight.shape, BF16),
            pltpu.VMEM((1, channels), F32),
            pltpu.VMEM((1, qc), F32),
            pltpu.VMEM((1, channels), F32),
            dma((19,)),
            pltpu.VMEM((4, span, width), BF16),
            pltpu.VMEM((span, width // nt), BF16),
            pltpu.VMEM((2, *kv_weights[0].shape), BF16),
            pltpu.VMEM((kvc, width) if flip else (width, kvc), BF16),
            pltpu.VMEM((width, half), BF16),
            pltpu.VMEM((width, half), BF16),
            pltpu.VMEM((width, half), BF16),
            pltpu.VMEM((2, ng, 2 * span, 2 * kvc), BF16),
            pltpu.VMEM((2, 4 * span, half), F32),
            pltpu.VMEM((4, span, half), F32),
            pltpu.VMEM((4 * span + 8, half), F32),
            pltpu.VMEM((3, 8, half), F32),
            pltpu.VMEM((ng, 8, half), F32),
            pltpu.VMEM((2, 4, span, half), BF16),
            pltpu.VMEM((2, nt, rows, channels), BF16),
            pltpu.VMEM((rows, cols), F32),
            dma((4,)), dma((4, no - 1)), dma((4,)), dma, dma, dma((2,)), dma((3, nto - 1)), dma,
            dma, dma, dma((ng - 1,)), dma((ng - 1,)), dma((ng,)), dma((ng,)), dma, dma, dma((ng - 1,)), dma((ng - 1,)),
            dma, dma((2,)), dma, dma((2, nto)), dma((2, nto - 1)), dma, dma,
        ],
        compiler_params=pltpu.CompilerParams(
            collective_id=0, has_side_effects=True, vmem_limit_bytes=60 * 1024 * 1024
        ),
    )(
        inputs.reshape(rows, width), norm_gain.reshape(1, width), query_weight, *kv_weights,
        query_gain.reshape(1, head_dim), key_gain.reshape(1, head_dim), forget_cache,
        rec_in_weight, rec_gate_weight, conv_weight, decay_gate_weight, input_gate_weight,
        decay_param.reshape(1, channels), decay_extra.reshape(rows, channels),
        attn_out_gain.reshape(1, qc), rec_out_gain.reshape(1, channels), out_att_weight, out_rec_weight,
    )
    return out.reshape(seqs, span, cols)


def solution(mesh):
    return jax.shard_map(
        functools.partial(body, mesh.shape["sp"], mesh.shape["tp"]),
        mesh=mesh,
        in_specs=(
            P(None, "sp", None), P(), P("sp", "tp"), P("sp", "tp"), P("sp", "tp"), P(), P(),
            P(None, "tp", None), P("sp", "tp"), P("sp", "tp"), P(None, "tp"), P("tp", None, None),
            P("tp", None, None), P("tp"), P(None, "sp", "tp"), P("tp"), P("tp"), P("tp", None), P("tp", None),
        ),
        out_specs=P(None, "sp", "tp"),
        check_vma=False,
    )
```
